32 devices in a mesh: ep: 8 (over z, y), tp: 4 (over x, core).
Axes of the slice: x: 2, y: 2, z: 4, core: 2. Of those that a mesh axis runs over, the one named last changes fastest.
Arguments:
- queries: bfloat16 [2048, 1536], P('ep', 'tp'), may hold values from -6 to 6
- kv_latent: bfloat16 [2048, 512], P('ep'), may hold values from -6 to 6
- rope_key: bfloat16 [2048, 64], P('ep'), may hold values from -6 to 6
- latent_gain: float32 [512], replicated, may hold values from 0.1 to 1.9
- w_key_up: bfloat16 [512, 1024], P(None, 'tp'), may hold values from -0.25 to 0.25
- w_value_up: bfloat16 [512, 1024], P(None, 'tp'), may hold values from -0.25 to 0.25
- query_gain: float32 [192], replicated, may hold values from 0.1 to 1.9
- key_gain: float32 [128], replicated, may hold values from 0.1 to 1.9
- rope_gain: float32 [64], replicated, may hold values from 0.1 to 1.9
- out_gain: float32 [128], replicated, may hold values from 0.1 to 1.9
- moe_tokens: bfloat16 [2048, 2048], P('ep'), may hold values from -6 to 6
- moe_gain: float32 [2048], replicated, may hold values from 0.1 to 1.9
- routes: int32 [2048, 2], P('ep'), may hold values from 0 to 7, all different within a row; in each aligned block of 64 rows (0 to 63, 64 to 127, ...) at most 24 rows name the same one
- route_weights: float32 [2048, 2], P('ep'), may hold values from 0.25 to 1
- w_gate: bfloat16 [8, 2048, 3584], P('ep', None, 'tp'), may hold values from -0.125 to 0.125
- w_up: bfloat16 [8, 2048, 3584], P('ep', None, 'tp'), may hold values from -0.125 to 0.125
- w_down: bfloat16 [8, 3584, 2048], P('ep', 'tp'), may hold values from -0.09375 to 0.09375
Outputs:
- attended: bfloat16 [2048, 1024], P('ep', 'tp')
- moe_out: bfloat16 [2048, 2048], P(('ep', 'tp'))
The draws below stay inside these ranges and needn't reach their ends.
Inputs may be any that keep to these rules, and one draw needn't show every extreme that they name: `routes`: each row names 2 different experts of 0 to 7; in each aligned block of 64 rows no expert is named by more than 24 rows, and in some block one expert is named by exactly 24.
All inputs are finite; a program needn't handle non-finite values.
Results may differ from the reference program's by a relative error of at most 0.0071.
Values may be sent and summed in bfloat16 or wider, within the bound.
A program may use at most 128 MiB of HBM per device.

```python
import math
import jax
import jax.numpy as jnp
import numpy as np
from jax import lax

D = 2048
HEADS = 8
NOPE = 128
ROPE_DIM = 64
VHEAD = 128
LATENT = 512
FF = 3584
TOP = 2
EXPERTS = 8
SEQ = 2048
MOE_ROWS = 2048
Q_ROWS = 64
CAP = 24


def shard_levels(stream_key, extent, shards, least, largest):
    def one(dim, parts):
        heights = jax.random.uniform(jax.random.fold_in(jax.random.fold_in(stream_key, 6), dim), (parts,), jnp.float32, least / len(shards), largest / len(shards))
        return jnp.repeat(jnp.exp(heights), extent[dim] // parts).reshape((-1,) + (1,) * (len(extent) - dim - 1))

    level = one(*shards[0])
    for cut in shards[1:]:
        level = level * one(*cut)
    return level


def assign_block(key, own, number, rows, count, top, bound, lean):
    order = jax.random.permutation(key, count)
    heavy_load, ordinary = portions_of(count, rows * top, bound, lean, True), portions_of(count, rows * top, bound, lean, False)
    places = jnp.arange(count)

    def named(tallies, offset_by):
        used = int((tallies > 0).sum())
        fixed = max(1, used // 4)
        shifted = fixed + (places - fixed + offset_by * (used - fixed)) % max(1, count - fixed)
        return jnp.zeros((count,), jnp.int32).at[order[jnp.where(places < fixed, places, shifted)]].set(jnp.asarray(tallies, jnp.int32))

    tallies = jnp.where(number % 4 == 0, named(heavy_load, number // 4), named(ordinary, number - number // 4 - 1))
    mixed = jax.random.permutation(jax.random.fold_in(own, 3), count)
    giver, receiver = mixed[0:count // 2 * 2:2], mixed[1:count // 2 * 2:2]
    margin = jnp.minimum(tallies[giver] - 1, bound - tallies[receiver]) // 2
    margin = jnp.where((giver == order[0]) | (receiver == order[0]) | (tallies[receiver] == 0), 0, jnp.maximum(margin, 0))
    shifted = jax.random.randint(jax.random.fold_in(own, 4), (count // 2,), 0, 1 << 20) % (margin + 1)
    tallies = tallies.at[giver].add(-shifted).at[receiver].add(shifted)
    labels = jnp.searchsorted(jnp.cumsum(tallies), jnp.arange(rows * top), side="right").astype(jnp.int32)
    table = labels.reshape(top, rows).T
    table = table[jax.random.permutation(jax.random.fold_in(own, 1), rows)]
    offset_by = jax.random.randint(jax.random.fold_in(own, 2), (rows, 1), 0, top)
    return jnp.take_along_axis(table, (jnp.arange(top)[None, :] + offset_by) % top, axis=1)


def portions_of(number_of, total, most, skew, full):
    portions = [(1 << 20) // math.isqrt(standing ** skew) + 1 for standing in range(1, number_of + 1)]
    largest = most if full else min(most, max(-(-total // number_of), total * portions[0] // sum(portions)))
    least = 1 if total - largest >= number_of - 1 else 0
    given, surplus = [largest] + [least] * (number_of - 1), total - largest - least * (number_of - 1)
    while surplus > 0:
        movable = [i for i in range(1, number_of) if given[i] < largest] or [i for i in range(1, number_of) if given[i] < most]
        mass, remaining = sum([portions[i] for i in movable]), surplus
        for i in movable:
            addition = min(most - given[i], max(1, remaining * portions[i] // mass), surplus)
            given[i] = given[i] + addition
            surplus = surplus - addition
    return np.array(given)


def scatter_about(stream_key, dims, scale, limit, shards=(), held_as=jnp.bfloat16):
    drawn = scale * jax.random.normal(stream_key, dims, jnp.float32)
    if shards:
        drawn = drawn * shard_levels(stream_key, dims, shards, -0.22, 0.18)
    return jnp.clip(drawn, -limit, limit).astype(held_as)


def setup_inputs(seed: int = 0) -> dict:
    streams_of = jax.random.split(jax.random.key(seed), 18)
    queries = scatter_about(streams_of[0], (SEQ, HEADS * (NOPE + ROPE_DIM)), 1.0, 6.0, ((0, 8), (1, 4)))
    kv_latent = scatter_about(streams_of[1], (SEQ, LATENT), 1.0, 6.0, ((0, 8),))
    rope_key = scatter_about(streams_of[2], (SEQ, ROPE_DIM), 1.0, 6.0, ((0, 8),))
    latent_gain = jnp.clip(1.0 + 0.18 * jax.random.normal(streams_of[3], (LATENT,), jnp.float32), 0.1, 1.9)
    w_key_up = scatter_about(streams_of[4], (LATENT, HEADS * NOPE), LATENT ** -0.5, 0.25, ((1, 4),))
    w_value_up = scatter_about(streams_of[5], (LATENT, HEADS * VHEAD), LATENT ** -0.5, 0.25, ((1, 4),))
    query_gain = jnp.clip(1.0 + 0.18 * jax.random.normal(streams_of[6], (NOPE + ROPE_DIM,), jnp.float32), 0.1, 1.9)
    key_gain = jnp.clip(1.0 + 0.18 * jax.random.normal(streams_of[7], (NOPE,), jnp.float32), 0.1, 1.9)
    rope_gain = jnp.clip(1.0 + 0.18 * jax.random.normal(streams_of[8], (ROPE_DIM,), jnp.float32), 0.1, 1.9)
    out_gain = jnp.clip(1.0 + 0.18 * jax.random.normal(streams_of[9], (VHEAD,), jnp.float32), 0.1, 1.9)
    moe_tokens = scatter_about(streams_of[10], (MOE_ROWS, D), 1.0, 6.0, ((0, 8),))
    moe_gain = jnp.clip(1.0 + 0.18 * jax.random.normal(streams_of[11], (D,), jnp.float32), 0.1, 1.9)
    routes_keys = jax.random.split(jax.random.fold_in(streams_of[12], 1), MOE_ROWS // Q_ROWS)
    routes_turns = jax.random.permutation(jax.random.fold_in(streams_of[12], 3), MOE_ROWS // Q_ROWS)
    routes = jax.vmap(lambda own, number: assign_block(jax.random.fold_in(streams_of[12], 2), own, number, Q_ROWS, EXPERTS, TOP, CAP, 1))(routes_keys, routes_turns).reshape((MOE_ROWS, TOP))
    route_weights = jnp.clip(0.25 + 0.75 * jax.random.uniform(streams_of[13], (MOE_ROWS, TOP), jnp.float32) ** shard_levels(streams_of[13], (MOE_ROWS, TOP), ((0, 8),), -0.2, 0.2), 0.25, 1.0)
    w_gate = scatter_about(streams_of[14], (EXPERTS, D, FF), D ** -0.5, 0.125, ((0, 8), (2, 4)))
    w_up = scatter_about(streams_of[15], (EXPERTS, D, FF), D ** -0.5, 0.125, ((0, 8), (2, 4)))
    w_down = scatter_about(streams_of[16], (EXPERTS, FF, D), FF ** -0.5, 0.09375, ((0, 8), (1, 4)))
    return {"queries": queries, "kv_latent": kv_latent, "rope_key": rope_key, "latent_gain": latent_gain, "w_key_up": w_key_up, "w_value_up": w_value_up, "query_gain": query_gain, "key_gain": key_gain, "rope_gain": rope_gain, "out_gain": out_gain, "moe_tokens": moe_tokens, "moe_gain": moe_gain, "routes": routes, "route_weights": route_weights, "w_gate": w_gate, "w_up": w_up, "w_down": w_down}


EPS = 1e-06
THETA = 500000.0

def rms_norm(values, norm_gain):
    return values * lax.rsqrt(lax.optimization_barrier(jnp.mean(values * values, axis=-1, keepdims=True)) + EPS) * norm_gain

def rounded(values):
    return lax.optimization_barrier(values.astype(jnp.bfloat16))

def rope_tables(positions, rope_dim):
    freqs = 1.0 / THETA ** (jnp.arange(0, rope_dim, 2, dtype=jnp.float32) / rope_dim)
    angles = positions.astype(jnp.float32)[:, None] * freqs[None, :]
    return (jnp.cos(angles), jnp.sin(angles))

def rotate(values, rot_cos, rot_sin):
    half_dim = values.shape[-1] // 2
    first_half = values[..., :half_dim]
    second_half = values[..., half_dim:]
    return jnp.concatenate([first_half * rot_cos - second_half * rot_sin, second_half * rot_cos + first_half * rot_sin], axis=-1)

def attention(queries, kv_latent, rope_key, latent_gain, w_key_up, w_value_up, query_gain, key_gain, rope_gain, out_gain):
    seq_len = queries.shape[0]
    positions = jnp.arange(seq_len, dtype=jnp.int32)
    rot_cos, rot_sin = rope_tables(positions, ROPE_DIM)
    latent = rounded(rms_norm(kv_latent.astype(jnp.float32), latent_gain))
    key_nope = jnp.dot(latent, w_key_up, preferred_element_type=jnp.float32).reshape(seq_len, HEADS, NOPE)
    key_nope = rounded(rms_norm(key_nope, key_gain)).astype(jnp.float32)
    values = rounded(jnp.dot(latent, w_value_up, preferred_element_type=jnp.float32))
    values = values.astype(jnp.float32).reshape(seq_len, HEADS, VHEAD)
    rot_key = rounded(rotate(rms_norm(rope_key.astype(jnp.float32), rope_gain), rot_cos, rot_sin)).astype(jnp.float32)
    query = rms_norm(queries.astype(jnp.float32).reshape(seq_len, HEADS, NOPE + ROPE_DIM), query_gain)
    query_nope = rounded(query[..., :NOPE]).astype(jnp.float32)
    query_rope = rounded(rotate(query[..., NOPE:], rot_cos[:, None, :], rot_sin[:, None, :])).astype(jnp.float32)
    scale = (NOPE + ROPE_DIM) ** (-0.5)
    block_rows = math.gcd(seq_len, 512)

    def one_block(block_index):
        block_first = block_index * block_rows
        q_nope = lax.dynamic_slice_in_dim(query_nope, block_first, block_rows, 0)
        q_rope = lax.dynamic_slice_in_dim(query_rope, block_first, block_rows, 0)
        scores = (jnp.einsum('qhd,khd->hqk', q_nope, key_nope, precision=lax.Precision.HIGHEST) + jnp.einsum('qhr,kr->hqk', q_rope, rot_key, precision=lax.Precision.HIGHEST)) * scale
        query_pos = block_first + jnp.arange(block_rows, dtype=jnp.int32)
        visible = (query_pos[:, None] >= positions[None, :])[None]
        exp_scores = jnp.where(visible, jnp.exp(scores), 0.0)
        denominator = lax.optimization_barrier(jnp.sum(exp_scores, axis=-1))
        weighted = jnp.einsum('hqk,khd->qhd', rounded(exp_scores).astype(jnp.float32), values, precision=lax.Precision.HIGHEST)
        mixed = weighted / jnp.transpose(denominator)[:, :, None]
        return rms_norm(mixed, out_gain).astype(jnp.bfloat16).reshape(block_rows, HEADS * VHEAD)
    blocks = lax.map(one_block, jnp.arange(seq_len // block_rows, dtype=jnp.int32))
    return blocks.reshape(seq_len, HEADS * VHEAD)

def experts_layer(moe_tokens, moe_gain, routes, route_weights, w_gate, w_up, w_down):
    n_rows = moe_tokens.shape[0]
    normed = rounded(rms_norm(moe_tokens.astype(jnp.float32), moe_gain))
    n_blocks = n_rows // Q_ROWS
    assigned = Q_ROWS * TOP
    slot_count = EXPERTS * CAP
    chosen = routes.reshape(n_blocks, assigned)
    onehot = (chosen[..., None] == jnp.arange(EXPERTS, dtype=jnp.int32)).astype(jnp.int32)
    rank = lax.optimization_barrier(jnp.sum((jnp.cumsum(onehot, axis=1) - onehot) * onehot, axis=-1)).astype(jnp.int32)
    slots = chosen * CAP + rank
    row_ids = jnp.arange(n_blocks, dtype=jnp.int32)[:, None] * Q_ROWS + jnp.arange(assigned, dtype=jnp.int32)[None, :] // TOP
    slot_hit = (slots[..., None] == jnp.arange(slot_count, dtype=jnp.int32)).astype(jnp.int32)
    table = lax.optimization_barrier(jnp.sum(slot_hit * (row_ids[..., None] + 1), axis=1)) - 1
    table = jnp.where(table < 0, n_rows, table).astype(jnp.int32)
    padded = jnp.concatenate([normed, jnp.zeros((1, normed.shape[1]), jnp.bfloat16)], axis=0)

    def one_expert(expert):
        rows_used = lax.dynamic_slice_in_dim(table, expert * CAP, CAP, 1).reshape(-1)
        inputs = padded[rows_used]
        gate = jnp.dot(inputs, w_gate[expert], preferred_element_type=jnp.float32)
        upward = jnp.dot(inputs, w_up[expert], preferred_element_type=jnp.float32)
        hidden = (jax.nn.silu(gate) * upward).astype(jnp.bfloat16)
        return rounded(jnp.dot(hidden, w_down[expert], preferred_element_type=jnp.float32))
    outputs = lax.map(one_expert, jnp.arange(EXPERTS, dtype=jnp.int32))
    place = jnp.arange(n_blocks, dtype=jnp.int32)[:, None] * CAP + rank
    picked = outputs[chosen, place].astype(jnp.float32)
    scaled = picked * route_weights.reshape(n_blocks, assigned)[..., None]
    mixed = lax.optimization_barrier(jnp.sum(scaled.reshape(n_rows, TOP, picked.shape[-1]), axis=1))
    return mixed.astype(jnp.bfloat16)

def reference(queries, kv_latent, rope_key, latent_gain, w_key_up, w_value_up, query_gain, key_gain, rope_gain, out_gain, moe_tokens, moe_gain, routes, route_weights, w_gate, w_up, w_down):
    attended = attention(queries, kv_latent, rope_key, latent_gain, w_key_up, w_value_up, query_gain, key_gain, rope_gain, out_gain)
    moe_out = experts_layer(moe_tokens, moe_gain, routes, route_weights, w_gate, w_up, w_down)
    return (attended, moe_out)
```

```python
import functools
import math

import jax
import jax.numpy as jnp
from jax import lax
from jax.experimental import pallas as pl
from jax.experimental.pallas import tpu as pltpu
from jax.sharding import PartitionSpec as P

EPS = 1e-06
THETA = 500000.0


def rms_norm(values, norm_gain):
    return values * lax.rsqrt(jnp.mean(values * values, axis=-1, keepdims=True) + EPS) * norm_gain


def rope_tables(positions, rope_dim):
    freqs = 1.0 / THETA ** (jnp.arange(0, rope_dim, 2, dtype=jnp.float32) / rope_dim)
    angles = positions.astype(jnp.float32)[:, None] * freqs[None, :]
    return (jnp.cos(angles), jnp.sin(angles))


def rotate(values, rot_cos, rot_sin):
    half_dim = values.shape[-1] // 2
    first_half = values[..., :half_dim]
    second_half = values[..., half_dim:]
    return jnp.concatenate(
        [
            first_half * rot_cos - second_half * rot_sin,
            second_half * rot_cos + first_half * rot_sin,
        ],
        axis=-1,
    )

MESH = pl.DeviceIdType.MESH
VMEM = pltpu.VMEM


def remote(src, dst, send, recv, device):
    return pltpu.make_async_remote_copy(
        src_ref=src, dst_ref=dst, send_sem=send, recv_sem=recv, device_id=device, device_id_type=MESH
    )


def greet(me, quarter, n_ep, highs):
    high, low = quarter // 2, quarter % 2
    barrier = pltpu.get_barrier_semaphore()

    def hello(device):
        pl.semaphore_signal(barrier, inc=1, device_id=device, device_id_type=MESH)

    def hello_ep(step, carry):
        hello((lax.rem(me + step, n_ep), quarter))
        return carry

    lax.fori_loop(1, n_ep, hello_ep, 0)
    hello((me, high * 2 + 1 - low))
    for step in range(1, highs):
        hello((me, lax.rem(high + step, highs) * 2 + low))
    pl.semaphore_wait(barrier, n_ep - 1 + 1 + highs - 1)


def spread_kernel(
    n_ep, highs, rows_ref, lat_ref, arrived, lat_all,
    own_sem, ep_send, ep_recv, high_send, high_recv, low_send, low_recv,
):
    me, quarter = lax.axis_index("ep"), lax.axis_index("tp")
    high, low = quarter // 2, quarter % 2
    partner = (me, high * 2 + 1 - low)
    greet(me, quarter, n_ep, highs)
    payloads = (
        (lambda j: rows_ref.at[j], arrived),
        (lambda j: lat_ref, lat_all),
    )
    own = [
        pltpu.make_async_copy(outgoing(me), into.at[low, high, me], own_sem.at[p])
        for p, (outgoing, into) in enumerate(payloads)
    ]
    for copy in own:
        copy.start()

    def ep_copy(p, step):
        outgoing, into = payloads[p]
        j = lax.rem(me + step, n_ep)
        return remote(
            outgoing(j), into.at[low, high, me], ep_send.at[p, step], ep_recv.at[p, step], (j, quarter)
        )

    def ep_arrival(p, step):
        outgoing, into = payloads[p]
        j = lax.rem(me + n_ep - step, n_ep)
        return remote(
            outgoing(me), into.at[low, high, j], ep_send.at[p, step], ep_recv.at[p, step], (j, quarter)
        )

    def high_copy(p, step, hop):
        into = payloads[p][1]
        j = lax.rem(me + n_ep - step, n_ep)
        block = into.at[low, high, j]
        return remote(
            block, block, high_send.at[p, hop, step], high_recv.at[p, hop, step],
            (me, lax.rem(high + hop, highs) * 2 + low),
        )

    def high_arrival(p, step, hop):
        into = payloads[p][1]
        j = lax.rem(me + n_ep - step, n_ep)
        block = into.at[low, lax.rem(high + highs - hop, highs), j]
        return remote(
            block, block, high_send.at[p, hop, step], high_recv.at[p, hop, step],
            (me, lax.rem(high + hop, highs) * 2 + low),
        )

    def low_copy(p, step, hop, side):
        into = payloads[p][1]
        j = lax.rem(me + n_ep - step, n_ep)
        block = into.at[side, lax.rem(high + highs - hop, highs), j]
        return remote(block, block, low_send.at[p, hop, step], low_recv.at[p, hop, step], partner)

    def start_ep(step, carry, p):
        ep_copy(p, step).start()
        return carry

    def forward(step, carry, p):
        ep_arrival(p, step).wait_recv()
        for hop in range(1, highs):
            high_copy(p, step, hop).start()
        low_copy(p, step, 0, low).start()
        return carry

    def forward_low(step, carry, p):
        for hop in range(1, highs):
            high_arrival(p, step, hop).wait_recv()
            low_copy(p, step, hop, low).start()
        return carry

    def finish(step, carry, p):
        for hop in range(highs):
            low_copy(p, step, hop, 1 - low).wait_recv()
            low_copy(p, step, hop, low).wait_send()
        for hop in range(1, highs):
            high_copy(p, step, hop).wait_send()
        return carry

    def finish_ep(step, carry, p):
        ep_copy(p, step).wait_send()
        return carry

    for p in range(2):
        lax.fori_loop(1, n_ep, functools.partial(start_ep, p=p), 0)
    for p in range(2):
        own[p].wait()
        for hop in range(1, highs):
            high_copy(p, 0, hop).start()
        low_copy(p, 0, 0, low).start()
        lax.fori_loop(1, n_ep, functools.partial(forward, p=p), 0)
    for p in range(2):
        lax.fori_loop(0, n_ep, functools.partial(forward_low, p=p), 0)
    for p in range(2):
        lax.fori_loop(0, n_ep, functools.partial(finish, p=p), 0)
        lax.fori_loop(1, n_ep, functools.partial(finish_ep, p=p), 0)


def spread(rows, lat, quarters):
    n_ep, cap, model_dim = rows.shape
    highs = quarters // 2
    dma = pltpu.SemaphoreType.DMA
    return pl.pallas_call(
        functools.partial(spread_kernel, n_ep, highs),
        out_shape=(
            jax.ShapeDtypeStruct((2, highs, n_ep, cap, model_dim), rows.dtype),
            jax.ShapeDtypeStruct((2, highs, n_ep) + lat.shape, lat.dtype),
        ),
        in_specs=[pl.BlockSpec(memory_space=VMEM)] * 2,
        out_specs=(pl.BlockSpec(memory_space=VMEM),) * 2,
        scratch_shapes=[
            dma((2,)),
            dma((2, n_ep)),
            dma((2, n_ep)),
            dma((2, highs, n_ep)),
            dma((2, highs, n_ep)),
            dma((2, highs, n_ep)),
            dma((2, highs, n_ep)),
        ],
        compiler_params=pltpu.CompilerParams(
            collective_id=0, has_side_effects=True, vmem_limit_bytes=60 << 20
        ),
        name="spread",
    )(rows, lat)


def collect_kernel(
    n_ep, highs, part_ref, ret, low_buf, high_buf, sum_buf, final_buf,
    low_send, low_recv, high_send, high_recv, ep_send, ep_recv,
):
    me, quarter = lax.axis_index("ep"), lax.axis_index("tp")
    high, low = quarter // 2, quarter % 2
    partner = (me, high * 2 + 1 - low)
    greet(me, quarter, n_ep, highs)

    def low_copy(step):
        j = lax.rem(me + step, n_ep)
        return remote(
            part_ref.at[1 - low, j], low_buf.at[j], low_send.at[step], low_recv.at[step], partner
        )

    def high_copy(step, hop):
        j = lax.rem(me + step, n_ep)
        other = lax.rem(high + hop, highs)
        return remote(
            sum_buf.at[j, other], high_buf.at[hop, j], high_send.at[hop, step],
            high_recv.at[hop, step], (me, other * 2 + low),
        )

    def ep_copy(step):
        j = lax.rem(me + step, n_ep)
        return remote(final_buf.at[j], ret.at[me], ep_send.at[step], ep_recv.at[step], (j, quarter))

    def ep_arrival(step):
        j = lax.rem(me + n_ep - step, n_ep)
        return remote(final_buf.at[j], ret.at[j], ep_send.at[step], ep_recv.at[step], (j, quarter))

    def start_low(step, carry):
        low_copy(step).start()
        return carry

    def add_low(step, carry):
        low_copy(step).wait_recv()
        j = lax.rem(me + step, n_ep)
        sum_buf[j] = (
            part_ref[low, j].astype(jnp.float32) + low_buf[j].astype(jnp.float32)
        ).astype(jnp.bfloat16)
        for hop in range(1, highs):
            high_copy(step, hop).start()
        return carry

    def total(step):
        j = lax.rem(me + step, n_ep)
        value = part_ref[low, j, high].astype(jnp.float32) + low_buf[j, high].astype(jnp.float32)
        for hop in range(1, highs):
            high_copy(step, hop).wait_recv()
            value = value + high_buf[hop, j].astype(jnp.float32)
        return value.astype(jnp.bfloat16)

    def add_high(step, carry):
        final_buf[lax.rem(me + step, n_ep)] = total(step)
        ep_copy(step).start()
        return carry

    def finish(step, carry):
        ep_arrival(step).wait_recv()
        ep_copy(step).wait_send()
        return carry

    def finish_tp(step, carry):
        low_copy(step).wait_send()
        for hop in range(1, highs):
            high_copy(step, hop).wait_send()
        return carry

    lax.fori_loop(1, n_ep, start_low, 0)
    low_copy(0).start()
    lax.fori_loop(1, n_ep, add_low, 0)
    add_low(0, 0)
    lax.fori_loop(1, n_ep, add_high, 0)
    ret[me] = total(0)
    lax.fori_loop(1, n_ep, finish, 0)
    lax.fori_loop(0, n_ep, finish_tp, 0)


def collect(partial):
    _, n_ep, highs, cap, model_dim = partial.shape
    dma = pltpu.SemaphoreType.DMA
    kind = partial.dtype
    return pl.pallas_call(
        functools.partial(collect_kernel, n_ep, highs),
        out_shape=jax.ShapeDtypeStruct((n_ep, cap, model_dim), kind),
        in_specs=[pl.BlockSpec(memory_space=VMEM)],
        out_specs=pl.BlockSpec(memory_space=VMEM),
        scratch_shapes=[
            VMEM((n_ep, highs, cap, model_dim), kind),
            VMEM((highs, n_ep, cap, model_dim), kind),
            VMEM((n_ep, highs, cap, model_dim), kind),
            VMEM((n_ep, cap, model_dim), kind),
            dma((n_ep,)),
            dma((n_ep,)),
            dma((highs, n_ep)),
            dma((highs, n_ep)),
            dma((n_ep,)),
            dma((n_ep,)),
        ],
        compiler_params=pltpu.CompilerParams(
            collective_id=1, has_side_effects=True, vmem_limit_bytes=62 << 20
        ),
        name="collect",
    )(partial)


def attend_kernel(
    heads, nope_dim, value_dim, latent_dim, scale,
    lat_ref, wk_ref, wv_ref, qn_ref, qr_ref, kg_ref, og_ref, out_ref, acc, den,
):
    block = pl.program_id(0)
    block_rows = lat_ref.shape[0]
    tok_rows = qn_ref.shape[1]
    offset = lax.axis_index("ep") * tok_rows
    first = block * block_rows

    @pl.when(block == 0)
    def _():
        acc[...] = jnp.zeros_like(acc)
        den[...] = jnp.zeros_like(den)

    @pl.when(first <= offset + tok_rows - 1)
    def _():
        latent = lat_ref[:, :latent_dim]
        rot_key = lat_ref[:, latent_dim:]
        keys = jnp.dot(latent, wk_ref[...], preferred_element_type=jnp.float32)
        values = jnp.dot(latent, wv_ref[...], preferred_element_type=jnp.float32).astype(jnp.bfloat16)
        shape = (tok_rows, block_rows)
        visible = offset + lax.broadcasted_iota(jnp.int32, shape, 0) >= first + lax.broadcasted_iota(
            jnp.int32, shape, 1
        )
        across = (((1,), (1,)), ((), ()))
        for head in range(heads):
            key = keys[:, head * nope_dim : (head + 1) * nope_dim]
            key = rms_norm(key, kg_ref[...]).astype(jnp.bfloat16)
            scores = lax.dot_general(qn_ref[head], key, across, preferred_element_type=jnp.float32)
            scores = scores + lax.dot_general(
                qr_ref[head], rot_key, across, preferred_element_type=jnp.float32
            )
            weights = jnp.where(visible, jnp.exp(scores * scale), 0.0)
            den[head] += jnp.sum(weights, axis=-1, keepdims=True)
            acc[head] += jnp.dot(
                weights.astype(jnp.bfloat16),
                values[:, head * value_dim : (head + 1) * value_dim],
                preferred_element_type=jnp.float32,
            )

    @pl.when(block == pl.num_programs(0) - 1)
    def _():
        for head in range(heads):
            mixed = rms_norm(acc[head] / den[head], og_ref[...])
            out_ref[:, head * value_dim : (head + 1) * value_dim] = mixed.astype(jnp.bfloat16)


def attend(lat_rows, w_key_up, w_value_up, query_nope, query_rope, key_gain, out_gain):
    heads, tok_rows, nope_dim = query_nope.shape
    rope_dim = query_rope.shape[2]
    value_dim = out_gain.shape[0]
    total, width = lat_rows.shape
    block_rows = math.gcd(total, 512)
    whole = pl.BlockSpec(memory_space=VMEM)
    return pl.pallas_call(
        functools.partial(
            attend_kernel, heads, nope_dim, value_dim, width - rope_dim, (nope_dim + rope_dim) ** (-0.5)
        ),
        grid=(total // block_rows,),
        out_shape=jax.ShapeDtypeStruct((tok_rows, heads * value_dim), jnp.bfloat16),
        in_specs=[pl.BlockSpec((block_rows, width), lambda b: (b, 0))] + [whole] * 6,
        out_specs=pl.BlockSpec((tok_rows, heads * value_dim), lambda b: (0, 0)),
        scratch_shapes=[
            VMEM((heads, tok_rows, value_dim), jnp.float32),
            VMEM((heads, tok_rows, 1), jnp.float32),
        ],
        name="attend",
    )(
        lat_rows, w_key_up, w_value_up, query_nope, query_rope,
        key_gain.reshape(1, -1), out_gain.reshape(1, -1),
    )


LANES = 128
TILE = 256


def layer_kernel(
    n_ep, heads, nope_dim, rope_dim, value_dim,
    q_ref, kv_ref, rk_ref, cos_ref, sin_ref, lg_ref, wk_ref, wv_ref, qg_ref, kg_ref, rg_ref, og_ref,
    tok_ref, mg_ref, routes_ref, rw_ref, wg_hbm, wu_hbm, wd_hbm,
    att_ref, moe_ref,
    wgu, wd, rows_out, arrived, hid, part, low_buf, sum_buf, high_buf, final_buf, ret, hits,
    lat_all, qn, qr, acc, den,
    w_sem, ep_send, ep_recv, high_send, high_recv, low_send, low_recv,
    rlow_send, rlow_recv, rhigh_send, rhigh_recv, rep_send, rep_recv,
    lz_send, lz_recv, ly_send, ly_recv, ll_send, ll_recv,
):
    me, quarter = lax.axis_index("ep"), lax.axis_index("tp")
    n_z = n_ep // 2
    z, y = me // 2, lax.rem(me, 2)
    high, low = quarter // 2, lax.rem(quarter, 2)
    partner = (me, high * 2 + 1 - low)
    across = (me, (1 - high) * 2 + low)
    bf16, f32 = jnp.bfloat16, jnp.float32
    cap = rows_out.shape[1]
    model_dim = rows_out.shape[2]
    tok_rows = tok_ref.shape[0]
    part_rows = tok_rows // 4
    ff = wd.shape[0]
    barrier = pltpu.get_barrier_semaphore()

    def hello(device):
        pl.semaphore_signal(barrier, inc=1, device_id=device, device_id_type=MESH)

    def hello_ep(step, carry):
        hello((lax.rem(me + step, n_ep), quarter))
        return carry

    lax.fori_loop(1, n_ep, hello_ep, 0)
    hello(partner)
    hello(across)

    def weight_copies():
        out = []
        for i in range(ff // LANES):
            out.append((wg_hbm.at[0, :, pl.ds(LANES * i, LANES)], wgu.at[:, pl.ds(TILE * i, LANES)]))
            out.append((wu_hbm.at[0, :, pl.ds(LANES * i, LANES)], wgu.at[:, pl.ds(TILE * i + LANES, LANES)]))
        out.append((wd_hbm.at[0], wd))
        return [pltpu.make_async_copy(a, b, w_sem.at[i]) for i, (a, b) in enumerate(out)]

    for copy in weight_copies():
        copy.start()

    def ep_to(s, t):
        return lax.rem(z + s, n_z) * 2 + lax.rem(y + t, 2)

    def ep_from(s, t):
        return lax.rem(z + n_z - s, n_z) * 2 + lax.rem(y + t, 2)


    def normed_rows(q):
        rows = tok_ref[pl.ds(pl.multiple_of(q * part_rows, part_rows), part_rows), :].astype(f32)
        return rms_norm(rows, mg_ref[...]).astype(bf16)

    def earlier_matrix():
        shape = (part_rows, part_rows)
        return (lax.broadcasted_iota(jnp.int32, shape, 0) > lax.broadcasted_iota(jnp.int32, shape, 1)).astype(bf16)

    def own_routes(q):
        return routes_ref[pl.ds(pl.multiple_of(q * part_rows, part_rows), part_rows), :]

    def dispatch():
        chosen = own_routes(quarter)
        experts = lax.broadcasted_iota(jnp.int32, (part_rows, LANES), 1)
        ones = [(chosen[:, k : k + 1] == experts).astype(f32) for k in range(2)]
        rank = jnp.dot(earlier_matrix(), (ones[0] + ones[1]).astype(bf16), preferred_element_type=f32)
        slot_ids = lax.broadcasted_iota(jnp.int32, (part_rows, n_ep * cap), 1).astype(f32)
        for k in range(2):
            own_rank = jnp.sum(rank * ones[k], axis=-1, keepdims=True)
            slot = chosen[:, k : k + 1].astype(f32) * cap + own_rank
            hits[k] = (slot_ids == slot).astype(bf16)
        select = (hits[0].astype(f32) + hits[1].astype(f32)).astype(bf16)
        rows = normed_rows(quarter)
        wide = 512
        for n in range(model_dim // wide):
            picked = lax.dot_general(
                select, rows[:, n * wide : (n + 1) * wide], (((0,), (0,)), ((), ())), preferred_element_type=f32
            )
            rows_out[:, :, n * wide : (n + 1) * wide] = picked.astype(bf16).reshape(n_ep, cap, wide)

    def own_dispatch(q, carry):
        chosen = own_routes(q)
        names = jnp.sum((chosen == me).astype(f32), axis=-1, keepdims=True)
        named = jnp.broadcast_to(names, (part_rows, LANES))
        rank = jnp.dot(earlier_matrix(), named.astype(bf16), preferred_element_type=f32)
        slot_ids = lax.broadcasted_iota(jnp.int32, (part_rows, LANES), 1).astype(f32)
        select = jnp.where(slot_ids == rank, named, 0.0).astype(bf16)[:, :cap]
        picked = lax.dot_general(
            select, normed_rows(q), (((0,), (0,)), ((), ())), preferred_element_type=f32
        )
        arrived[me, lax.rem(q, 2), q // 2] = picked.astype(bf16)
        return carry

    dispatch()
    pl.semaphore_wait(barrier, n_ep + 1)

    def ep_copy(s, t):
        return remote(
            rows_out.at[ep_to(s, t)], arrived.at[me, low, high], ep_send.at[s, t], ep_recv.at[s, t],
            (ep_to(s, t), quarter),
        )

    def ep_arrival(s, t):
        j = ep_from(s, t)
        return remote(
            rows_out.at[j], arrived.at[j, low, high], ep_send.at[s, t], ep_recv.at[s, t], (j, quarter)
        )

    def high_copy(s, t, side):
        block = arrived.at[ep_from(s, t), low, side]
        return remote(block, block, high_send.at[s, t], high_recv.at[s, t], across)

    def low_copy(s, t, hop, side, core):
        block = arrived.at[ep_from(s, t), core, side]
        return remote(block, block, low_send.at[hop, s, t], low_recv.at[hop, s, t], partner)

    def each(s, body):
        for t in range(2):
            if t == 0:
                pl.when(s > 0)(functools.partial(body, s, 0))
            else:
                body(s, 1)

    def start_ep(s, carry):
        each(s, lambda s, t: ep_copy(s, t).start())
        return carry

    lax.fori_loop(1, n_z, start_ep, 0)
    start_ep(0, 0)


    def lat_copy_z(k):
        block = lat_all.at[k, y, low]
        return remote(
            block, block, lz_send.at[k], lz_recv.at[k], (lax.rem(z + 1, n_z) * 2 + y, quarter)
        )

    def lat_copy_y(k, side):
        block = lat_all.at[k, side, low]
        return remote(block, block, ly_send.at[k], ly_recv.at[k], (z * 2 + 1 - y, quarter))

    def lat_copy_low(k, hop, core):
        block = lat_all.at[k, y if hop == 0 else 1 - y, core]
        return remote(block, block, ll_send.at[hop, k], ll_recv.at[hop, k], partner)

    def lat_own():
        latent = rms_norm(kv_ref[...].astype(f32), lg_ref[...]).astype(bf16)
        rot = rotate(rms_norm(rk_ref[...].astype(f32), rg_ref[...]), cos_ref[...], sin_ref[...]).astype(bf16)
        half = tok_rows // 2
        width = latent.shape[1]
        for core in range(2):
            lat_all[z, y, core, :, :width] = latent[core * half : (core + 1) * half]
            lat_all[z, y, core, :, width:] = rot[core * half : (core + 1) * half]
        pl.when(z < n_z - 1)(lambda: lat_copy_z(z).start())
        pl.when(y == 0)(lambda: lat_copy_y(z, y).start())

    def lat_step(k, carry):
        origin = z - k

        @pl.when(origin >= 0)
        def _():
            lat_copy_z(origin).wait_recv()
            pl.when(z < n_z - 1)(lambda: lat_copy_z(origin).start())
            lat_copy_y(origin, y).start()
            lat_copy_low(origin, 0, low).start()

        return carry

    def lat_side(k, carry):
        origin = z - k

        @pl.when((origin >= 0) & (k + y > 0))
        def _():
            lat_copy_y(origin, 1 - y).wait_recv()
            lat_copy_low(origin, 1, low).start()

        return carry


    def queries():
        raw = q_ref[...].astype(f32)
        width = nope_dim + rope_dim
        for head in range(heads):
            query = rms_norm(raw[:, head * width : (head + 1) * width], qg_ref[...])
            qn[head] = query[:, :nope_dim].astype(bf16)
            qr[head] = rotate(query[:, nope_dim:], cos_ref[...], sin_ref[...]).astype(bf16)

    scale = (nope_dim + rope_dim) ** (-0.5)

    def attend_block(zj, yj, own):
        block = lat_all[zj, yj].reshape(tok_rows, lat_all.shape[-1])
        width = block.shape[1] - rope_dim
        latent, rot_key = block[:, :width], block[:, width:]
        keys = jnp.dot(latent, wk_ref[...], preferred_element_type=f32)
        values = jnp.dot(latent, wv_ref[...], preferred_element_type=f32).astype(bf16)
        lined = (((1,), (1,)), ((), ()))
        for head in range(heads):
            key = rms_norm(keys[:, head * nope_dim : (head + 1) * nope_dim], kg_ref[...]).astype(bf16)
            scores = lax.dot_general(qn[head], key, lined, preferred_element_type=f32)
            scores = scores + lax.dot_general(qr[head], rot_key, lined, preferred_element_type=f32)
            weights = jnp.exp(scores * scale)
            if own:
                shape = (tok_rows, tok_rows)
                visible = lax.broadcasted_iota(jnp.int32, shape, 0) >= lax.broadcasted_iota(jnp.int32, shape, 1)
                weights = jnp.where(visible, weights, 0.0)
            total = jnp.sum(weights, axis=-1, keepdims=True)
            mixed = jnp.dot(
                weights.astype(bf16), values[:, head * value_dim : (head + 1) * value_dim],
                preferred_element_type=f32,
            )
            if own:
                den[head] = total
                acc[head] = mixed
            else:
                den[head] += total
                acc[head] += mixed

    def attend_side(k):
        @pl.when((z >= k) & (k + y > 0))
        def _():
            lat_copy_low(z - k, 1, 1 - low).wait_recv()
            attend_block(z - k, 1 - y, False)

    def attend_line(k):
        @pl.when(z >= k)
        def _():
            lat_copy_low(z - k, 0, 1 - low).wait_recv()
            attend_block(z - k, y, False)


    def forward(s, t):
        ep_arrival(s, t).wait_recv()
        high_copy(s, t, high).start()
        low_copy(s, t, 0, high, low).start()

    def forward_low(s, t):
        high_copy(s, t, 1 - high).wait_recv()
        low_copy(s, t, 1, 1 - high, low).start()

    def arrive(s, t):
        low_copy(s, t, 0, high, 1 - low).wait_recv()
        low_copy(s, t, 1, 1 - high, 1 - low).wait_recv()

    def expert(s):
        first = lax.rem(z + n_z - s, n_z) * 2
        rows = arrived[pl.ds(first, 2)].reshape(8 * cap, model_dim)
        for i in range(ff // LANES):
            both = jnp.dot(rows, wgu[:, TILE * i : TILE * (i + 1)], preferred_element_type=f32)
            gate, upward = both[:, :LANES], both[:, LANES:]
            hid[:, LANES * i : LANES * (i + 1)] = (jax.nn.silu(gate) * upward).astype(bf16)
        for n in range(model_dim // TILE):
            down = jnp.dot(hid[...], wd[:, TILE * n : TILE * (n + 1)], preferred_element_type=f32)
            part[pl.ds(first, 2), :, :, :, TILE * n : TILE * (n + 1)] = down.astype(bf16).reshape(
                2, 2, 2, cap, TILE
            )

    def rlow_copy(s, t):
        j = ep_from(s, t)
        return remote(part.at[j, 1 - low], low_buf.at[j], rlow_send.at[s, t], rlow_recv.at[s, t], partner)

    def rhigh_copy(s, t):
        j = ep_from(s, t)
        return remote(sum_buf.at[j], high_buf.at[j], rhigh_send.at[s, t], rhigh_recv.at[s, t], across)

    def rep_copy(s, t):
        j = ep_from(s, t)
        return remote(final_buf.at[j], ret.at[me], rep_send.at[s, t], rep_recv.at[s, t], (j, quarter))

    def rep_arrival(s, t):
        j = ep_to(s, t)
        return remote(final_buf.at[j], ret.at[j], rep_send.at[s, t], rep_recv.at[s, t], (j, quarter))

    def reduce_low(s):
        for t in range(2):
            j = ep_from(s, t)
            rlow_copy(s, t).wait_recv()
            sum_buf[j] = (part[j, low, 1 - high].astype(f32) + low_buf[j, 1 - high].astype(f32)).astype(bf16)
            rhigh_copy(s, t).start()

    def reduce_high(s):
        for t in range(2):
            j = ep_from(s, t)
            rhigh_copy(s, t).wait_recv()
            value = part[j, low, high].astype(f32) + low_buf[j, high].astype(f32) + high_buf[j].astype(f32)
            value = value.astype(bf16)
            if t == 0:

                @pl.when(s == 0)
                def _():
                    ret[me] = value

                @pl.when(s > 0)
                def _():
                    final_buf[j] = value
                    rep_copy(s, 0).start()
            else:
                final_buf[j] = value
                rep_copy(s, 1).start()

    lax.fori_loop(0, 4, own_dispatch, 0)
    lat_own()
    queries()
    attend_block(z, y, True)

    def stage(s, carry):
        each(s, forward)
        each(s, forward_low)
        each(s, arrive)

        @pl.when(s == 0)
        def _():
            for copy in weight_copies():
                copy.wait()

        expert(s)
        for t in range(2):
            rlow_copy(s, t).start()
        pl.when(s > 0)(lambda: reduce_low(s - 1))
        pl.when(s > 1)(lambda: reduce_high(s - 2))
        return carry

    lax.fori_loop(0, n_z, stage, 0)
    lax.fori_loop(1, n_z, lat_step, 0)
    reduce_low(n_z - 1)
    reduce_high(n_z - 2)
    lax.fori_loop(0, n_z, lat_side, 0)
    reduce_high(n_z - 1)

    def attend_step(k, carry):
        pl.when(k > 0)(lambda: attend_line(k))
        attend_side(k)
        return carry

    lax.fori_loop(0, n_z, attend_step, 0)
    for head in range(heads):
        mixed = rms_norm(acc[head] / den[head], og_ref[...])
        att_ref[:, head * value_dim : (head + 1) * value_dim] = mixed.astype(bf16)

    def returned(s, carry):
        each(s, lambda s, t: rep_arrival(s, t).wait_recv())
        return carry

    lax.fori_loop(0, n_z, returned, 0)
    weights = rw_ref[pl.ds(pl.multiple_of(quarter * part_rows, part_rows), part_rows), :]
    wide = 512
    for n in range(model_dim // wide):
        values = ret[:, :, n * wide : (n + 1) * wide].reshape(n_ep * cap, wide)
        mixed = jnp.dot(hits[0], values, preferred_element_type=f32) * weights[:, 0:1]
        mixed += jnp.dot(hits[1], values, preferred_element_type=f32) * weights[:, 1:2]
        moe_ref[:, n * wide : (n + 1) * wide] = mixed.astype(bf16)

    def sent(s, carry):
        def rows_sent(s, t):
            ep_copy(s, t).wait_send()
            high_copy(s, t, high).wait_send()
            low_copy(s, t, 0, high, low).wait_send()
            low_copy(s, t, 1, 1 - high, low).wait_send()
            rep_copy(s, t).wait_send()

        each(s, rows_sent)
        for t in range(2):
            rlow_copy(s, t).wait_send()
            rhigh_copy(s, t).wait_send()

        origin = z - s

        @pl.when(origin >= 0)
        def _():
            pl.when(z < n_z - 1)(lambda: lat_copy_z(origin).wait_send())
            pl.when((s > 0) | (y == 0))(lambda: lat_copy_y(origin, y).wait_send())
            pl.when(s > 0)(lambda: lat_copy_low(origin, 0, low).wait_send())
            pl.when(s + y > 0)(lambda: lat_copy_low(origin, 1, low).wait_send())

        return carry

    lax.fori_loop(0, n_z, sent, 0)


def layer(
    queries, kv_latent, rope_key, rot_cos, rot_sin, latent_gain, w_key_up, w_value_up, query_gain, key_gain,
    rope_gain, out_gain, moe_tokens, moe_gain, routes, route_weights, w_gate, w_up, w_down, n_ep, cap,
):
    tok_rows = queries.shape[0]
    nope_dim, rope_dim, value_dim = key_gain.shape[0], rope_key.shape[1], out_gain.shape[0]
    heads = w_key_up.shape[1] // nope_dim
    model_dim = moe_tokens.shape[1]
    part_rows = tok_rows // 4
    ff = w_down.shape[1]
    n_z = n_ep // 2
    width = kv_latent.shape[1] + rope_dim
    dma = pltpu.SemaphoreType.DMA
    kind = jnp.bfloat16
    pairs = (n_z, 2)
    block = (cap, model_dim)
    vmem, anywhere = pl.BlockSpec(memory_space=VMEM), pl.BlockSpec(memory_space=pl.ANY)
    return pl.pallas_call(
        functools.partial(layer_kernel, n_ep, heads, nope_dim, rope_dim, value_dim),
        out_shape=(
            jax.ShapeDtypeStruct((tok_rows, heads * value_dim), kind),
            jax.ShapeDtypeStruct((part_rows, model_dim), kind),
        ),
        in_specs=[vmem] * 16 + [anywhere] * 3,
        out_specs=(vmem, vmem),
        scratch_shapes=[
            VMEM((model_dim, 2 * ff), kind),
            VMEM((ff, model_dim), kind),
            VMEM((n_ep,) + block, kind),
            VMEM((n_ep, 2, 2) + block, kind),
            VMEM((8 * cap, ff), kind),
            VMEM((n_ep, 2, 2) + block, kind),
            VMEM((n_ep, 2) + block, kind),
            VMEM((n_ep,) + block, kind),
            VMEM((n_ep,) + block, kind),
            VMEM((n_ep,) + block, kind),
            VMEM((n_ep,) + block, kind),
            VMEM((2, part_rows, n_ep * cap), kind),
            VMEM((n_z, 2, 2, tok_rows // 2, width), kind),
            VMEM((heads, tok_rows, nope_dim), kind),
            VMEM((heads, tok_rows, rope_dim), kind),
            VMEM((heads, tok_rows, value_dim), jnp.float32),
            VMEM((heads, tok_rows, 1), jnp.float32),
            dma((2 * (ff // LANES) + 1,)),
            dma(pairs), dma(pairs), dma(pairs), dma(pairs), dma((2,) + pairs), dma((2,) + pairs),
            dma(pairs), dma(pairs), dma(pairs), dma(pairs), dma(pairs), dma(pairs),
            dma((n_z,)), dma((n_z,)), dma((n_z,)), dma((n_z,)), dma((2, n_z)), dma((2, n_z)),
        ],
        compiler_params=pltpu.CompilerParams(
            collective_id=2, has_side_effects=True, vmem_limit_bytes=62 << 20
        ),
        name="layer",
    )(
        queries, kv_latent, rope_key, rot_cos, rot_sin, latent_gain.reshape(1, -1), w_key_up, w_value_up,
        query_gain.reshape(1, -1), key_gain.reshape(1, -1), rope_gain.reshape(1, -1), out_gain.reshape(1, -1),
        moe_tokens, moe_gain.reshape(1, -1), routes, route_weights, w_gate, w_up, w_down,
    )


def on_device(
    queries,
    kv_latent,
    rope_key,
    latent_gain,
    w_key_up,
    w_value_up,
    query_gain,
    key_gain,
    rope_gain,
    out_gain,
    moe_tokens,
    moe_gain,
    routes,
    route_weights,
    w_gate,
    w_up,
    w_down,
):
    quarters = lax.axis_size("tp")
    n_ep = lax.axis_size("ep")
    my_part = lax.axis_index("tp")
    tok_rows = queries.shape[0]
    nope_dim = key_gain.shape[0]
    value_dim = out_gain.shape[0]
    rope_dim = rope_key.shape[1]
    head_count = w_key_up.shape[1] // nope_dim
    positions = lax.axis_index("ep") * tok_rows + jnp.arange(tok_rows, dtype=jnp.int32)
    rot_cos, rot_sin = rope_tables(positions, rope_dim)
    n_rows, model_dim = moe_tokens.shape
    top_count = routes.shape[1]
    part_rows = n_rows // quarters
    experts = n_ep * w_gate.shape[0]
    capacity = (3 * top_count * part_rows + 2 * experts - 1) // (2 * experts)
    one_kernel = quarters == 4 and n_ep % 2 == 0 and w_gate.shape[0] == 1 and top_count == 2
    if one_kernel and capacity % 8 == 0 and w_down.shape[1] % LANES == 0 and model_dim % 512 == 0:
        return layer(
            queries, kv_latent, rope_key, rot_cos, rot_sin, latent_gain, w_key_up, w_value_up, query_gain,
            key_gain, rope_gain, out_gain, moe_tokens, moe_gain, routes, route_weights, w_gate, w_up, w_down,
            n_ep, capacity,
        )
    lat_part = tok_rows // quarters

    def mine(values, rows):
        return lax.dynamic_slice_in_dim(values, my_part * rows, rows, 0)

    latent = rms_norm(mine(kv_latent, lat_part).astype(jnp.float32), latent_gain)
    rot_key = rotate(
        rms_norm(mine(rope_key, lat_part).astype(jnp.float32), rope_gain),
        mine(rot_cos, lat_part),
        mine(rot_sin, lat_part),
    )
    lat_own = jnp.concatenate([latent.astype(jnp.bfloat16), rot_key.astype(jnp.bfloat16)], axis=1)

    slot_count = experts * capacity
    own_rows = rms_norm(mine(moe_tokens, part_rows).astype(jnp.float32), moe_gain).astype(jnp.bfloat16)
    chosen = mine(routes, part_rows).reshape(part_rows * top_count)
    onehot = (chosen[:, None] == jnp.arange(experts, dtype=jnp.int32)).astype(jnp.float32)
    count = part_rows * top_count
    earlier = (jnp.arange(count)[:, None] > jnp.arange(count)[None, :]).astype(jnp.float32)
    rank = jnp.sum(jnp.dot(earlier, onehot) * onehot, axis=-1).astype(jnp.int32)
    slots = chosen * capacity + rank
    mine_hit = (slots[:, None] == jnp.arange(slot_count, dtype=jnp.int32)).astype(jnp.bfloat16)
    mine_hit = mine_hit.reshape(part_rows, top_count, slot_count)
    outgoing = jnp.einsum(
        "rs,rd->sd", jnp.sum(mine_hit, axis=1), own_rows, preferred_element_type=jnp.float32
    )
    outgoing = outgoing.astype(jnp.bfloat16).reshape(experts, capacity, model_dim)

    arrived, lat_all = spread(outgoing, lat_own, quarters)
    lat_rows = jnp.transpose(lat_all, (2, 1, 0, 3, 4)).reshape(n_ep * tok_rows, lat_own.shape[1])

    shape = arrived.shape
    gate = jnp.einsum("abecd,df->abecf", arrived, w_gate[0], preferred_element_type=jnp.float32)
    upward = jnp.einsum("abecd,df->abecf", arrived, w_up[0], preferred_element_type=jnp.float32)
    hidden = (jax.nn.silu(gate) * upward).astype(jnp.bfloat16)
    partial = jnp.einsum("abecf,fd->aebcd", hidden, w_down[0], preferred_element_type=jnp.float32)
    returned = collect(partial.astype(jnp.bfloat16))

    query = rms_norm(
        queries.astype(jnp.float32).reshape(tok_rows, head_count, nope_dim + rope_dim), query_gain
    )
    query_nope = query[..., :nope_dim].astype(jnp.bfloat16)
    query_rope = rotate(query[..., nope_dim:], rot_cos[:, None, :], rot_sin[:, None, :]).astype(
        jnp.bfloat16
    )
    attended = attend(
        lat_rows,
        w_key_up,
        w_value_up,
        jnp.transpose(query_nope, (1, 0, 2)),
        jnp.transpose(query_rope, (1, 0, 2)),
        key_gain,
        out_gain,
    )

    picked = jnp.einsum(
        "rks,sd->rkd",
        mine_hit,
        returned.reshape(slot_count, model_dim),
        preferred_element_type=jnp.float32,
    )
    own_weights = mine(route_weights, part_rows)
    moe_out = jnp.sum(picked * own_weights[:, :, None], axis=1).astype(jnp.bfloat16)
    return (attended, moe_out)


def solution(mesh):
    return jax.shard_map(
        on_device,
        mesh=mesh,
        in_specs=(
            P("ep", "tp"),
            P("ep", None),
            P("ep", None),
            P(),
            P(None, "tp"),
            P(None, "tp"),
            P(),
            P(),
            P(),
            P(),
            P("ep", None),
            P(),
            P("ep", None),
            P("ep", None),
            P("ep", None, "tp"),
            P("ep", None, "tp"),
            P("ep", "tp", None),
        ),
        out_specs=(P("ep", "tp"), P(("ep", "tp"), None)),
        check_vma=False,
    )
```

```python
import functools
import math

import jax
import jax.numpy as jnp
from jax import lax
from jax.experimental import pallas as pl
from jax.experimental.pallas import tpu as pltpu
from jax.sharding import PartitionSpec as P

EPS = 1e-06
THETA = 500000.0


def rms_norm(values, norm_gain):
    return values * lax.rsqrt(jnp.mean(values * values, axis=-1, keepdims=True) + EPS) * norm_gain


def rope_tables(positions, rope_dim):
    freqs = 1.0 / THETA ** (jnp.arange(0, rope_dim, 2, dtype=jnp.float32) / rope_dim)
    angles = positions.astype(jnp.float32)[:, None] * freqs[None, :]
    return (jnp.cos(angles), jnp.sin(angles))


def rotate(values, rot_cos, rot_sin):
    half_dim = values.shape[-1] // 2
    first_half = values[..., :half_dim]
    second_half = values[..., half_dim:]
    return jnp.concatenate(
        [
            first_half * rot_cos - second_half * rot_sin,
            second_half * rot_cos + first_half * rot_sin,
        ],
        axis=-1,
    )

MESH = pl.DeviceIdType.MESH
VMEM = pltpu.VMEM


def remote(src, dst, send, recv, device):
    return pltpu.make_async_remote_copy(
        src_ref=src, dst_ref=dst, send_sem=send, recv_sem=recv, device_id=device, device_id_type=MESH
    )


def greet(me, quarter, n_ep, highs):
    high, low = quarter // 2, quarter % 2
    barrier = pltpu.get_barrier_semaphore()

    def hello(device):
        pl.semaphore_signal(barrier, inc=1, device_id=device, device_id_type=MESH)

    def hello_ep(step, carry):
        hello((lax.rem(me + step, n_ep), quarter))
        return carry

    lax.fori_loop(1, n_ep, hello_ep, 0)
    hello((me, high * 2 + 1 - low))
    for step in range(1, highs):
        hello((me, lax.rem(high + step, highs) * 2 + low))
    pl.semaphore_wait(barrier, n_ep - 1 + 1 + highs - 1)


def spread_kernel(
    n_ep, highs, rows_ref, lat_ref, arrived, lat_all,
    own_sem, ep_send, ep_recv, high_send, high_recv, low_send, low_recv,
):
    me, quarter = lax.axis_index("ep"), lax.axis_index("tp")
    high, low = quarter // 2, quarter % 2
    partner = (me, high * 2 + 1 - low)
    greet(me, quarter, n_ep, highs)
    payloads = (
        (lambda j: rows_ref.at[j], arrived),
        (lambda j: lat_ref, lat_all),
    )
    own = [
        pltpu.make_async_copy(outgoing(me), into.at[low, high, me], own_sem.at[p])
        for p, (outgoing, into) in enumerate(payloads)
    ]
    for copy in own:
        copy.start()

    def ep_copy(p, step):
        outgoing, into = payloads[p]
        j = lax.rem(me + step, n_ep)
        return remote(
            outgoing(j), into.at[low, high, me], ep_send.at[p, step], ep_recv.at[p, step], (j, quarter)
        )

    def ep_arrival(p, step):
        outgoing, into = payloads[p]
        j = lax.rem(me + n_ep - step, n_ep)
        return remote(
            outgoing(me), into.at[low, high, j], ep_send.at[p, step], ep_recv.at[p, step], (j, quarter)
        )

    def high_copy(p, step, hop):
        into = payloads[p][1]
        j = lax.rem(me + n_ep - step, n_ep)
        block = into.at[low, high, j]
        return remote(
            block, block, high_send.at[p, hop, step], high_recv.at[p, hop, step],
            (me, lax.rem(high + hop, highs) * 2 + low),
        )

    def high_arrival(p, step, hop):
        into = payloads[p][1]
        j = lax.rem(me + n_ep - step, n_ep)
        block = into.at[low, lax.rem(high + highs - hop, highs), j]
        return remote(
            block, block, high_send.at[p, hop, step], high_recv.at[p, hop, step],
            (me, lax.rem(high + hop, highs) * 2 + low),
        )

    def low_copy(p, step, hop, side):
        into = payloads[p][1]
        j = lax.rem(me + n_ep - step, n_ep)
        block = into.at[side, lax.rem(high + highs - hop, highs), j]
        return remote(block, block, low_send.at[p, hop, step], low_recv.at[p, hop, step], partner)

    def start_ep(step, carry, p):
        ep_copy(p, step).start()
        return carry

    def forward(step, carry, p):
        ep_arrival(p, step).wait_recv()
        for hop in range(1, highs):
            high_copy(p, step, hop).start()
        low_copy(p, step, 0, low).start()
        return carry

    def forward_low(step, carry, p):
        for hop in range(1, highs):
            high_arrival(p, step, hop).wait_recv()
            low_copy(p, step, hop, low).start()
        return carry

    def finish(step, carry, p):
        for hop in range(highs):
            low_copy(p, step, hop, 1 - low).wait_recv()
            low_copy(p, step, hop, low).wait_send()
        for hop in range(1, highs):
            high_copy(p, step, hop).wait_send()
        return carry

    def finish_ep(step, carry, p):
        ep_copy(p, step).wait_send()
        return carry

    for p in range(2):
        lax.fori_loop(1, n_ep, functools.partial(start_ep, p=p), 0)
    for p in range(2):
        own[p].wait()
        for hop in range(1, highs):
            high_copy(p, 0, hop).start()
        low_copy(p, 0, 0, low).start()
        lax.fori_loop(1, n_ep, functools.partial(forward, p=p), 0)
    for p in range(2):
        lax.fori_loop(0, n_ep, functools.partial(forward_low, p=p), 0)
    for p in range(2):
        lax.fori_loop(0, n_ep, functools.partial(finish, p=p), 0)
        lax.fori_loop(1, n_ep, functools.partial(finish_ep, p=p), 0)


def spread(rows, lat, quarters):
    n_ep, cap, model_dim = rows.shape
    highs = quarters // 2
    dma = pltpu.SemaphoreType.DMA
    return pl.pallas_call(
        functools.partial(spread_kernel, n_ep, highs),
        out_shape=(
            jax.ShapeDtypeStruct((2, highs, n_ep, cap, model_dim), rows.dtype),
            jax.ShapeDtypeStruct((2, highs, n_ep) + lat.shape, lat.dtype),
        ),
        in_specs=[pl.BlockSpec(memory_space=VMEM)] * 2,
        out_specs=(pl.BlockSpec(memory_space=VMEM),) * 2,
        scratch_shapes=[
            dma((2,)),
            dma((2, n_ep)),
            dma((2, n_ep)),
            dma((2, highs, n_ep)),
            dma((2, highs, n_ep)),
            dma((2, highs, n_ep)),
            dma((2, highs, n_ep)),
        ],
        compiler_params=pltpu.CompilerParams(
            collective_id=0, has_side_effects=True, vmem_limit_bytes=60 << 20
        ),
        name="spread",
    )(rows, lat)


def collect_kernel(
    n_ep, highs, part_ref, ret, low_buf, high_buf, sum_buf, final_buf,
    low_send, low_recv, high_send, high_recv, ep_send, ep_recv,
):
    me, quarter = lax.axis_index("ep"), lax.axis_index("tp")
    high, low = quarter // 2, quarter % 2
    partner = (me, high * 2 + 1 - low)
    greet(me, quarter, n_ep, highs)

    def low_copy(step):
        j = lax.rem(me + step, n_ep)
        return remote(
            part_ref.at[1 - low, j], low_buf.at[j], low_send.at[step], low_recv.at[step], partner
        )

    def high_copy(step, hop):
        j = lax.rem(me + step, n_ep)
        other = lax.rem(high + hop, highs)
        return remote(
            sum_buf.at[j, other], high_buf.at[hop, j], high_send.at[hop, step],
            high_recv.at[hop, step], (me, other * 2 + low),
        )

    def ep_copy(step):
        j = lax.rem(me + step, n_ep)
        return remote(final_buf.at[j], ret.at[me], ep_send.at[step], ep_recv.at[step], (j, quarter))

    def ep_arrival(step):
        j = lax.rem(me + n_ep - step, n_ep)
        return remote(final_buf.at[j], ret.at[j], ep_send.at[step], ep_recv.at[step], (j, quarter))

    def start_low(step, carry):
        low_copy(step).start()
        return carry

    def add_low(step, carry):
        low_copy(step).wait_recv()
        j = lax.rem(me + step, n_ep)
        sum_buf[j] = (
            part_ref[low, j].astype(jnp.float32) + low_buf[j].astype(jnp.float32)
        ).astype(jnp.bfloat16)
        for hop in range(1, highs):
            high_copy(step, hop).start()
        return carry

    def total(step):
        j = lax.rem(me + step, n_ep)
        value = part_ref[low, j, high].astype(jnp.float32) + low_buf[j, high].astype(jnp.float32)
        for hop in range(1, highs):
            high_copy(step, hop).wait_recv()
            value = value + high_buf[hop, j].astype(jnp.float32)
        return value.astype(jnp.bfloat16)

    def add_high(step, carry):
        final_buf[lax.rem(me + step, n_ep)] = total(step)
        ep_copy(step).start()
        return carry

    def finish(step, carry):
        ep_arrival(step).wait_recv()
        ep_copy(step).wait_send()
        return carry

    def finish_tp(step, carry):
        low_copy(step).wait_send()
        for hop in range(1, highs):
            high_copy(step, hop).wait_send()
        return carry

    lax.fori_loop(1, n_ep, start_low, 0)
    low_copy(0).start()
    lax.fori_loop(1, n_ep, add_low, 0)
    add_low(0, 0)
    lax.fori_loop(1, n_ep, add_high, 0)
    ret[me] = total(0)
    lax.fori_loop(1, n_ep, finish, 0)
    lax.fori_loop(0, n_ep, finish_tp, 0)


def collect(partial):
    _, n_ep, highs, cap, model_dim = partial.shape
    dma = pltpu.SemaphoreType.DMA
    kind = partial.dtype
    return pl.pallas_call(
        functools.partial(collect_kernel, n_ep, highs),
        out_shape=jax.ShapeDtypeStruct((n_ep, cap, model_dim), kind),
        in_specs=[pl.BlockSpec(memory_space=VMEM)],
        out_specs=pl.BlockSpec(memory_space=VMEM),
        scratch_shapes=[
            VMEM((n_ep, highs, cap, model_dim), kind),
            VMEM((highs, n_ep, cap, model_dim), kind),
            VMEM((n_ep, highs, cap, model_dim), kind),
            VMEM((n_ep, cap, model_dim), kind),
            dma((n_ep,)),
            dma((n_ep,)),
            dma((highs, n_ep)),
            dma((highs, n_ep)),
            dma((n_ep,)),
            dma((n_ep,)),
        ],
        compiler_params=pltpu.CompilerParams(
            collective_id=1, has_side_effects=True, vmem_limit_bytes=62 << 20
        ),
        name="collect",
    )(partial)


def attend_kernel(
    heads, nope_dim, value_dim, latent_dim, scale,
    lat_ref, wk_ref, wv_ref, qn_ref, qr_ref, kg_ref, og_ref, out_ref, acc, den,
):
    block = pl.program_id(0)
    block_rows = lat_ref.shape[0]
    tok_rows = qn_ref.shape[1]
    offset = lax.axis_index("ep") * tok_rows
    first = block * block_rows

    @pl.when(block == 0)
    def _():
        acc[...] = jnp.zeros_like(acc)
        den[...] = jnp.zeros_like(den)

    @pl.when(first <= offset + tok_rows - 1)
    def _():
        latent = lat_ref[:, :latent_dim]
        rot_key = lat_ref[:, latent_dim:]
        keys = jnp.dot(latent, wk_ref[...], preferred_element_type=jnp.float32)
        values = jnp.dot(latent, wv_ref[...], preferred_element_type=jnp.float32).astype(jnp.bfloat16)
        shape = (tok_rows, block_rows)
        visible = offset + lax.broadcasted_iota(jnp.int32, shape, 0) >= first + lax.broadcasted_iota(
            jnp.int32, shape, 1
        )
        across = (((1,), (1,)), ((), ()))
        for head in range(heads):
            key = keys[:, head * nope_dim : (head + 1) * nope_dim]
            key = rms_norm(key, kg_ref[...]).astype(jnp.bfloat16)
            scores = lax.dot_general(qn_ref[head], key, across, preferred_element_type=jnp.float32)
            scores = scores + lax.dot_general(
                qr_ref[head], rot_key, across, preferred_element_type=jnp.float32
            )
            weights = jnp.where(visible, jnp.exp(scores * scale), 0.0)
            den[head] += jnp.sum(weights, axis=-1, keepdims=True)
            acc[head] += jnp.dot(
                weights.astype(jnp.bfloat16),
                values[:, head * value_dim : (head + 1) * value_dim],
                preferred_element_type=jnp.float32,
            )

    @pl.when(block == pl.num_programs(0) - 1)
    def _():
        for head in range(heads):
            mixed = rms_norm(acc[head] / den[head], og_ref[...])
            out_ref[:, head * value_dim : (head + 1) * value_dim] = mixed.astype(jnp.bfloat16)


def attend(lat_rows, w_key_up, w_value_up, query_nope, query_rope, key_gain, out_gain):
    heads, tok_rows, nope_dim = query_nope.shape
    rope_dim = query_rope.shape[2]
    value_dim = out_gain.shape[0]
    total, width = lat_rows.shape
    block_rows = math.gcd(total, 512)
    whole = pl.BlockSpec(memory_space=VMEM)
    return pl.pallas_call(
        functools.partial(
            attend_kernel, heads, nope_dim, value_dim, width - rope_dim, (nope_dim + rope_dim) ** (-0.5)
        ),
        grid=(total // block_rows,),
        out_shape=jax.ShapeDtypeStruct((tok_rows, heads * value_dim), jnp.bfloat16),
        in_specs=[pl.BlockSpec((block_rows, width), lambda b: (b, 0))] + [whole] * 6,
        out_specs=pl.BlockSpec((tok_rows, heads * value_dim), lambda b: (0, 0)),
        scratch_shapes=[
            VMEM((heads, tok_rows, value_dim), jnp.float32),
            VMEM((heads, tok_rows, 1), jnp.float32),
        ],
        name="attend",
    )(
        lat_rows, w_key_up, w_value_up, query_nope, query_rope,
        key_gain.reshape(1, -1), out_gain.reshape(1, -1),
    )


LANES = 128
TILE = 256


def layer_kernel(
    n_ep, heads, nope_dim, rope_dim, value_dim,
    tok_hbm, mg_hbm, routes_hbm, rw_hbm, kv_hbm, rk_hbm, freq_hbm, lg_hbm, rg_hbm, q_hbm, qg_hbm,
    wk_hbm, wv_hbm, kg_hbm, og_hbm, wg_hbm, wu_hbm, wd_hbm,
    att_ref, moe_ref,
    tok_ref, mg_ref, routes_ref, rw_ref, kv_ref, rk_ref, freq_ref, lg_ref, rg_ref, q_ref, qg_ref,
    wk_ref, wv_ref, kg_ref, og_ref,
    wgu, wd, normed, rows_out, arrived, hid, part, low_buf, sum_buf, high_buf, final_buf, ret, hits,
    lat_all, cos_ref, sin_ref, qn, qr, acc, den,
    in_sem, w_sem, ep_send, ep_recv, high_send, high_recv, low_send, low_recv,
    rlow_send, rlow_recv, rhigh_send, rhigh_recv, rep_send, rep_recv,
    lz_send, lz_recv, ly_send, ly_recv, ll_send, ll_recv,
):
    me, quarter = lax.axis_index("ep"), lax.axis_index("tp")
    n_z = n_ep // 2
    z, y = me // 2, lax.rem(me, 2)
    high, low = quarter // 2, lax.rem(quarter, 2)
    partner = (me, high * 2 + 1 - low)
    across = (me, (1 - high) * 2 + low)
    bf16, f32 = jnp.bfloat16, jnp.float32
    cap = rows_out.shape[1]
    model_dim = rows_out.shape[2]
    tok_rows = tok_ref.shape[0]
    part_rows = tok_rows // 4
    ff = wd.shape[0]
    barrier = pltpu.get_barrier_semaphore()

    def hello(device):
        pl.semaphore_signal(barrier, inc=1, device_id=device, device_id_type=MESH)

    def hello_ep(step, carry):
        hello((lax.rem(me + step, n_ep), quarter))
        return carry

    lax.fori_loop(1, n_ep, hello_ep, 0)
    hello(partner)
    hello(across)

    def weight_copies():
        out = []
        for i in range(ff // LANES):
            out.append((wg_hbm.at[0, :, pl.ds(LANES * i, LANES)], wgu.at[:, pl.ds(TILE * i, LANES)]))
            out.append((wu_hbm.at[0, :, pl.ds(LANES * i, LANES)], wgu.at[:, pl.ds(TILE * i + LANES, LANES)]))
        out.append((wd_hbm.at[0], wd))
        return [pltpu.make_async_copy(a, b, w_sem.at[i]) for i, (a, b) in enumerate(out)]

    sources = (
        tok_hbm, mg_hbm, routes_hbm, rw_hbm, kv_hbm, rk_hbm, freq_hbm, lg_hbm, rg_hbm, q_hbm, qg_hbm,
        wk_hbm, wv_hbm, kg_hbm, og_hbm,
    )
    loaded = (
        tok_ref, mg_ref, routes_ref, rw_ref, kv_ref, rk_ref, freq_ref, lg_ref, rg_ref, q_ref, qg_ref,
        wk_ref, wv_ref, kg_ref, og_ref,
    )
    loads = [
        pltpu.make_async_copy(source, into, in_sem.at[i])
        for i, (source, into) in enumerate(zip(sources, loaded))
    ]
    for copy in loads:
        copy.start()
    for copy in weight_copies():
        copy.start()

    def ep_to(s, t):
        return lax.rem(z + s, n_z) * 2 + lax.rem(y + t, 2)

    def ep_from(s, t):
        return lax.rem(z + n_z - s, n_z) * 2 + lax.rem(y + t, 2)


    tokens = (1, tok_rows)
    token = lax.broadcasted_iota(jnp.int32, tokens, 1)

    def quarter_of(index):
        return sum((index >= q * part_rows).astype(jnp.int32) for q in range(1, 4))

    def hit_matrix(count, places):
        slot = lax.broadcasted_iota(jnp.int32, (count, places[0].shape[1]), 0).astype(f32)
        return sum((slot == place).astype(f32) for place in places)

    def gather_rows(select, into):
        select = select.astype(bf16)
        wide = 512
        for n in range(model_dim // wide):
            cols = slice(n * wide, (n + 1) * wide)
            rows = jnp.dot(select, normed[:, cols], preferred_element_type=f32).astype(bf16)
            into(cols, rows, wide)

    def own_part(row):
        return sum(
            jnp.where(quarter == q, row[:, q * part_rows : (q + 1) * part_rows], 0.0) for q in range(4)
        )

    def ranks():
        shape = (tok_rows, tok_rows)
        before, after = lax.broadcasted_iota(jnp.int32, shape, 0), lax.broadcasted_iota(jnp.int32, shape, 1)
        earlier = ((before < after) & (quarter_of(before) == quarter_of(after))).astype(bf16)
        experts = lax.broadcasted_iota(jnp.int32, (n_ep, tok_rows), 0)
        ones = [(routes_ref[k : k + 1, :] == experts).astype(f32) for k in range(2)]
        rank = jnp.dot((ones[0] + ones[1]).astype(bf16), earlier, preferred_element_type=f32)
        return [jnp.sum(rank * one, axis=0, keepdims=True) for one in ones]

    def norm_tokens():
        step = 64
        for i in range(tok_rows // step):
            rows = tok_ref[i * step : (i + 1) * step, :].astype(f32)
            normed[i * step : (i + 1) * step, :] = rms_norm(rows, mg_ref[...]).astype(bf16)

    def dispatch(rank):
        mine = quarter_of(token) == quarter
        places = [
            jnp.where(mine, routes_ref[k : k + 1, :].astype(f32) * cap + rank[k], -1.0) for k in range(2)
        ]

        def into(cols, rows, wide):
            rows_out[:, :, cols] = rows.reshape(n_ep, cap, wide)

        gather_rows(hit_matrix(n_ep * cap, places), into)

    def own_dispatch(rank):
        number = quarter_of(token)
        position = lax.rem(number, 2) * 2 + number // 2
        places = [
            jnp.where(routes_ref[k : k + 1, :] == me, position.astype(f32) * cap + rank[k], -1.0)
            for k in range(2)
        ]

        def into(cols, rows, wide):
            arrived[me, :, :, :, cols] = rows.reshape(2, 2, cap, wide)

        gather_rows(hit_matrix(4 * cap, places), into)

    def combine_matrices(rank):
        slot = lax.broadcasted_iota(jnp.int32, (n_ep * cap, part_rows), 0).astype(f32)
        weighted = jnp.zeros((n_ep * cap, part_rows), f32)
        for k in range(2):
            place = own_part(routes_ref[k : k + 1, :].astype(f32) * cap + rank[k])
            weighted += jnp.where(slot == place, own_part(rw_ref[k : k + 1, :]), 0.0)
        upper = weighted.astype(bf16)
        hits[0] = upper
        hits[1] = (weighted - upper.astype(f32)).astype(bf16)

    for copy in loads[:4]:
        copy.wait()
    rank = ranks()
    norm_tokens()
    dispatch(rank)
    pl.semaphore_wait(barrier, n_ep + 1)

    def ep_copy(s, t):
        return remote(
            rows_out.at[ep_to(s, t)], arrived.at[me, low, high], ep_send.at[s, t], ep_recv.at[s, t],
            (ep_to(s, t), quarter),
        )

    def ep_arrival(s, t):
        j = ep_from(s, t)
        return remote(
            rows_out.at[j], arrived.at[j, low, high], ep_send.at[s, t], ep_recv.at[s, t], (j, quarter)
        )

    def high_copy(s, t, side):
        block = arrived.at[ep_from(s, t), low, side]
        return remote(block, block, high_send.at[s, t], high_recv.at[s, t], across)

    def low_copy(s, t, hop, side, core):
        block = arrived.at[ep_from(s, t), core, side]
        return remote(block, block, low_send.at[hop, s, t], low_recv.at[hop, s, t], partner)

    def each(s, body):
        for t in range(2):
            if t == 0:
                pl.when(s > 0)(functools.partial(body, s, 0))
            else:
                body(s, 1)

    def start_ep(s, carry):
        each(s, lambda s, t: ep_copy(s, t).start())
        return carry

    lax.fori_loop(1, n_z, start_ep, 0)
    start_ep(0, 0)


    def lat_copy_z(k):
        block = lat_all.at[k, y, low]
        return remote(
            block, block, lz_send.at[k], lz_recv.at[k], (lax.rem(z + 1, n_z) * 2 + y, quarter)
        )

    def lat_copy_y(k, side):
        block = lat_all.at[k, side, low]
        return remote(block, block, ly_send.at[k], ly_recv.at[k], (z * 2 + 1 - y, quarter))

    def lat_copy_low(k, hop, core):
        block = lat_all.at[k, y if hop == 0 else 1 - y, core]
        return remote(block, block, ll_send.at[hop, k], ll_recv.at[hop, k], partner)

    def tables():
        half_dim = rope_dim // 2
        places = lax.broadcasted_iota(jnp.int32, (tok_rows, half_dim), 0) + me * tok_rows
        angles = places.astype(f32) * freq_ref[...]
        cos_ref[...] = jnp.cos(angles)
        sin_ref[...] = jnp.sin(angles)

    def lat_own():
        latent = rms_norm(kv_ref[...].astype(f32), lg_ref[...]).astype(bf16)
        raw = jnp.transpose(rk_ref[...].astype(f32))
        rot = rotate(rms_norm(raw, rg_ref[...]), cos_ref[...], sin_ref[...]).astype(bf16)
        half = tok_rows // 2
        width = latent.shape[1]
        for core in range(2):
            lat_all[z, y, core, :, :width] = latent[core * half : (core + 1) * half]
            lat_all[z, y, core, :, width:] = rot[core * half : (core + 1) * half]
        pl.when(z < n_z - 1)(lambda: lat_copy_z(z).start())
        pl.when(y == 0)(lambda: lat_copy_y(z, y).start())

    def lat_step(k, carry):
        origin = z - k

        @pl.when(origin >= 0)
        def _():
            lat_copy_z(origin).wait_recv()
            pl.when(z < n_z - 1)(lambda: lat_copy_z(origin).start())
            lat_copy_y(origin, y).start()
            lat_copy_low(origin, 0, low).start()

        return carry

    def lat_side(k, carry):
        origin = z - k

        @pl.when((origin >= 0) & (k + y > 0))
        def _():
            lat_copy_y(origin, 1 - y).wait_recv()
            lat_copy_low(origin, 1, low).start()

        return carry


    def queries():
        raw = q_ref[...].astype(f32)
        width = nope_dim + rope_dim
        for head in range(heads):
            query = rms_norm(raw[:, head * width : (head + 1) * width], qg_ref[...])
            qn[head] = query[:, :nope_dim].astype(bf16)
            qr[head] = rotate(query[:, nope_dim:], cos_ref[...], sin_ref[...]).astype(bf16)

    scale = (nope_dim + rope_dim) ** (-0.5)

    def attend_block(zj, yj, own):
        block = lat_all[zj, yj].reshape(tok_rows, lat_all.shape[-1])
        width = block.shape[1] - rope_dim
        latent, rot_key = block[:, :width], block[:, width:]
        keys = jnp.dot(latent, wk_ref[...], preferred_element_type=f32)
        values = jnp.dot(latent, wv_ref[...], preferred_element_type=f32).astype(bf16)
        lined = (((1,), (1,)), ((), ()))
        for head in range(heads):
            key = rms_norm(keys[:, head * nope_dim : (head + 1) * nope_dim], kg_ref[...]).astype(bf16)
            scores = lax.dot_general(qn[head], key, lined, preferred_element_type=f32)
            scores = scores + lax.dot_general(qr[head], rot_key, lined, preferred_element_type=f32)
            weights = jnp.exp(scores * scale)
            if own:
                shape = (tok_rows, tok_rows)
                visible = lax.broadcasted_iota(jnp.int32, shape, 0) >= lax.broadcasted_iota(jnp.int32, shape, 1)
                weights = jnp.where(visible, weights, 0.0)
            total = jnp.sum(weights, axis=-1, keepdims=True)
            mixed = jnp.dot(
                weights.astype(bf16), values[:, head * value_dim : (head + 1) * value_dim],
                preferred_element_type=f32,
            )
            if own:
                den[head] = total
                acc[head] = mixed
            else:
                den[head] += total
                acc[head] += mixed

    def attend_side(k):
        @pl.when((z >= k) & (k + y > 0))
        def _():
            lat_copy_low(z - k, 1, 1 - low).wait_recv()
            attend_block(z - k, 1 - y, False)

    def attend_line(k):
        @pl.when(z >= k)
        def _():
            lat_copy_low(z - k, 0, 1 - low).wait_recv()
            attend_block(z - k, y, False)


    def forward(s, t):
        ep_arrival(s, t).wait_recv()
        high_copy(s, t, high).start()
        low_copy(s, t, 0, high, low).start()

    def forward_low(s, t):
        high_copy(s, t, 1 - high).wait_recv()
        low_copy(s, t, 1, 1 - high, low).start()

    def arrive(s, t):
        low_copy(s, t, 0, high, 1 - low).wait_recv()
        low_copy(s, t, 1, 1 - high, 1 - low).wait_recv()

    def expert(s):
        first = lax.rem(z + n_z - s, n_z) * 2
        rows = arrived[pl.ds(first, 2)].reshape(8 * cap, model_dim)
        for i in range(ff // LANES):
            both = jnp.dot(rows, wgu[:, TILE * i : TILE * (i + 1)], preferred_element_type=f32)
            gate, upward = both[:, :LANES], both[:, LANES:]
            hid[:, LANES * i : LANES * (i + 1)] = (jax.nn.silu(gate) * upward).astype(bf16)
        for n in range(model_dim // TILE):
            down = jnp.dot(hid[...], wd[:, TILE * n : TILE * (n + 1)], preferred_element_type=f32)
            part[pl.ds(first, 2), :, :, :, TILE * n : TILE * (n + 1)] = down.astype(bf16).reshape(
                2, 2, 2, cap, TILE
            )

    def rlow_copy(s, t):
        j = ep_from(s, t)
        return remote(part.at[j, 1 - low], low_buf.at[j], rlow_send.at[s, t], rlow_recv.at[s, t], partner)

    def rhigh_copy(s, t):
        j = ep_from(s, t)
        return remote(sum_buf.at[j], high_buf.at[j], rhigh_send.at[s, t], rhigh_recv.at[s, t], across)

    def rep_copy(s, t):
        j = ep_from(s, t)
        return remote(final_buf.at[j], ret.at[me], rep_send.at[s, t], rep_recv.at[s, t], (j, quarter))

    def rep_arrival(s, t):
        j = ep_to(s, t)
        return remote(final_buf.at[j], ret.at[j], rep_send.at[s, t], rep_recv.at[s, t], (j, quarter))

    def reduce_low(s):
        for t in range(2):
            j = ep_from(s, t)
            rlow_copy(s, t).wait_recv()
            sum_buf[j] = (part[j, low, 1 - high].astype(f32) + low_buf[j, 1 - high].astype(f32)).astype(bf16)
            rhigh_copy(s, t).start()

    def reduce_high(s):
        for t in range(2):
            j = ep_from(s, t)
            rhigh_copy(s, t).wait_recv()
            value = part[j, low, high].astype(f32) + low_buf[j, high].astype(f32) + high_buf[j].astype(f32)
            value = value.astype(bf16)
            if t == 0:

                @pl.when(s == 0)
                def _():
                    ret[me] = value

                @pl.when(s > 0)
                def _():
                    final_buf[j] = value
                    rep_copy(s, 0).start()
            else:
                final_buf[j] = value
                rep_copy(s, 1).start()

    def order(i):
        if n_z % 2:
            return i
        return jnp.where(i < n_z - 1, lax.rem(2 * i, n_z - 1), n_z - 1)

    def lat_hop(k):
        if k < n_z:
            lat_step(k, 0)

    def attend_step(k):
        if k < n_z:
            if k > 0:
                attend_line(k)
            attend_side(k)

    own_dispatch(rank)
    combine_matrices(rank)
    each(0, forward)
    for copy in loads[4:]:
        copy.wait()
    tables()
    lat_own()
    forward(order(1), 0)
    queries()
    attend_block(z, y, True)

    def stage(i, carry):
        s = order(i)
        each(s, forward_low)
        each(s, arrive)

        @pl.when(i == 0)
        def _():
            for copy in weight_copies():
                copy.wait()

        expert(s)
        for t in range(2):
            rlow_copy(s, t).start()

        @pl.when(i == 0)
        def _():
            forward(order(1), 1)
            each(order(2), forward)

        @pl.when((i > 0) & (i < n_z - 2))
        def _():
            reduce_low(s)
            each(order(i + 2), forward)

        @pl.when(i == n_z - 2)
        def _():
            lat_hop(1)
            reduce_low(s)

        @pl.when((i > 1) & (i < n_z - 1))
        def _():
            reduce_high(order(i - 1))

        return carry

    lax.fori_loop(0, n_z, stage, 0)
    lat_hop(2)
    last = order(n_z - 1)
    reduce_low(last)
    reduce_low(0)
    tail = [order(n_z - 2), last, 0]
    for k in range(n_z):
        lat_side(k, 0)
        if k == 1:
            for far in range(3, n_z):
                lat_hop(far)
        if 0 < k and tail:
            reduce_high(tail.pop(0))
        attend_step(k)
    for head in range(heads):
        mixed = rms_norm(acc[head] / den[head], og_ref[...])
        att_ref[:, head * value_dim : (head + 1) * value_dim] = mixed.astype(bf16)

    def returned(s, carry):
        each(s, lambda s, t: rep_arrival(s, t).wait_recv())
        return carry

    lax.fori_loop(0, n_z, returned, 0)
    wide = 512
    lined = (((0,), (0,)), ((), ()))
    for n in range(model_dim // wide):
        values = ret[:, :, n * wide : (n + 1) * wide].reshape(n_ep * cap, wide)
        mixed = lax.dot_general(hits[0], values, lined, preferred_element_type=f32)
        mixed += lax.dot_general(hits[1], values, lined, preferred_element_type=f32)
        moe_ref[:, n * wide : (n + 1) * wide] = mixed.astype(bf16)

    def sent(s, carry):
        def rows_sent(s, t):
            ep_copy(s, t).wait_send()
            high_copy(s, t, high).wait_send()
            low_copy(s, t, 0, high, low).wait_send()
            low_copy(s, t, 1, 1 - high, low).wait_send()
            rep_copy(s, t).wait_send()

        each(s, rows_sent)
        for t in range(2):
            rlow_copy(s, t).wait_send()
            rhigh_copy(s, t).wait_send()

        origin = z - s

        @pl.when(origin >= 0)
        def _():
            pl.when(z < n_z - 1)(lambda: lat_copy_z(origin).wait_send())
            pl.when((s > 0) | (y == 0))(lambda: lat_copy_y(origin, y).wait_send())
            pl.when(s > 0)(lambda: lat_copy_low(origin, 0, low).wait_send())
            pl.when(s + y > 0)(lambda: lat_copy_low(origin, 1, low).wait_send())

        return carry

    lax.fori_loop(0, n_z, sent, 0)


def layer(
    queries, kv_latent, rope_key, latent_gain, w_key_up, w_value_up, query_gain, key_gain,
    rope_gain, out_gain, moe_tokens, moe_gain, routes, route_weights, w_gate, w_up, w_down, n_ep, cap,
):
    tok_rows = queries.shape[0]
    nope_dim, rope_dim, value_dim = key_gain.shape[0], rope_key.shape[1], out_gain.shape[0]
    heads = w_key_up.shape[1] // nope_dim
    model_dim = moe_tokens.shape[1]
    part_rows = tok_rows // 4
    ff = w_down.shape[1]
    n_z = n_ep // 2
    width = kv_latent.shape[1] + rope_dim
    dma = pltpu.SemaphoreType.DMA
    kind, f32 = jnp.bfloat16, jnp.float32
    pairs = (n_z, 2)
    block = (cap, model_dim)
    freqs = 1.0 / THETA ** (jnp.arange(0, rope_dim, 2, dtype=f32) / rope_dim)
    small = (
        moe_tokens, moe_gain.reshape(1, -1), routes.T, route_weights.T, kv_latent, rope_key.T,
        freqs.reshape(1, -1), latent_gain.reshape(1, -1), rope_gain.reshape(1, -1), queries,
        query_gain.reshape(1, -1), w_key_up, w_value_up, key_gain.reshape(1, -1), out_gain.reshape(1, -1),
    )
    return pl.pallas_call(
        functools.partial(layer_kernel, n_ep, heads, nope_dim, rope_dim, value_dim),
        out_shape=(
            jax.ShapeDtypeStruct((tok_rows, heads * value_dim), kind),
            jax.ShapeDtypeStruct((part_rows, model_dim), kind),
        ),
        in_specs=[pl.BlockSpec(memory_space=pltpu.HBM)] * (len(small) + 3),
        out_specs=(pl.BlockSpec(memory_space=VMEM),) * 2,
        scratch_shapes=[VMEM(array.shape, array.dtype) for array in small] + [
            VMEM((model_dim, 2 * ff), kind),
            VMEM((ff, model_dim), kind),
            VMEM((tok_rows, model_dim), kind),
            VMEM((n_ep,) + block, kind),
            VMEM((n_ep, 2, 2) + block, kind),
            VMEM((8 * cap, ff), kind),
            VMEM((n_ep, 2, 2) + block, kind),
            VMEM((n_ep, 2) + block, kind),
            VMEM((n_ep,) + block, kind),
            VMEM((n_ep,) + block, kind),
            VMEM((n_ep,) + block, kind),
            VMEM((n_ep,) + block, kind),
            VMEM((2, n_ep * cap, part_rows), kind),
            VMEM((n_z, 2, 2, tok_rows // 2, width), kind),
            VMEM((tok_rows, rope_dim // 2), f32),
            VMEM((tok_rows, rope_dim // 2), f32),
            VMEM((heads, tok_rows, nope_dim), kind),
            VMEM((heads, tok_rows, rope_dim), kind),
            VMEM((heads, tok_rows, value_dim), f32),
            VMEM((heads, tok_rows, 1), f32),
            dma((len(small),)),
            dma((2 * (ff // LANES) + 1,)),
            dma(pairs), dma(pairs), dma(pairs), dma(pairs), dma((2,) + pairs), dma((2,) + pairs),
            dma(pairs), dma(pairs), dma(pairs), dma(pairs), dma(pairs), dma(pairs),
            dma((n_z,)), dma((n_z,)), dma((n_z,)), dma((n_z,)), dma((2, n_z)), dma((2, n_z)),
        ],
        compiler_params=pltpu.CompilerParams(
            collective_id=2, has_side_effects=True, vmem_limit_bytes=62 << 20
        ),
        name="layer",
    )(*small, w_gate, w_up, w_down)


def on_device(
    queries,
    kv_latent,
    rope_key,
    latent_gain,
    w_key_up,
    w_value_up,
    query_gain,
    key_gain,
    rope_gain,
    out_gain,
    moe_tokens,
    moe_gain,
    routes,
    route_weights,
    w_gate,
    w_up,
    w_down,
):
    quarters = lax.axis_size("tp")
    n_ep = lax.axis_size("ep")
    my_part = lax.axis_index("tp")
    tok_rows = queries.shape[0]
    nope_dim = key_gain.shape[0]
    value_dim = out_gain.shape[0]
    rope_dim = rope_key.shape[1]
    head_count = w_key_up.shape[1] // nope_dim
    positions = lax.axis_index("ep") * tok_rows + jnp.arange(tok_rows, dtype=jnp.int32)
    rot_cos, rot_sin = rope_tables(positions, rope_dim)
    n_rows, model_dim = moe_tokens.shape
    top_count = routes.shape[1]
    part_rows = n_rows // quarters
    experts = n_ep * w_gate.shape[0]
    capacity = (3 * top_count * part_rows + 2 * experts - 1) // (2 * experts)
    one_kernel = quarters == 4 and n_ep % 2 == 0 and w_gate.shape[0] == 1 and top_count == 2
    one_kernel = one_kernel and n_ep >= 8
    if one_kernel and capacity % 8 == 0 and w_down.shape[1] % LANES == 0 and model_dim % 512 == 0:
        return layer(
            queries, kv_latent, rope_key, latent_gain, w_key_up, w_value_up, query_gain, key_gain, rope_gain,
            out_gain, moe_tokens, moe_gain, routes, route_weights, w_gate, w_up, w_down, n_ep, capacity,
        )
    lat_part = tok_rows // quarters

    def mine(values, rows):
        return lax.dynamic_slice_in_dim(values, my_part * rows, rows, 0)

    latent = rms_norm(mine(kv_latent, lat_part).astype(jnp.float32), latent_gain)
    rot_key = rotate(
        rms_norm(mine(rope_key, lat_part).astype(jnp.float32), rope_gain),
        mine(rot_cos, lat_part),
        mine(rot_sin, lat_part),
    )
    lat_own = jnp.concatenate([latent.astype(jnp.bfloat16), rot_key.astype(jnp.bfloat16)], axis=1)

    slot_count = experts * capacity
    own_rows = rms_norm(mine(moe_tokens, part_rows).astype(jnp.float32), moe_gain).astype(jnp.bfloat16)
    chosen = mine(routes, part_rows).reshape(part_rows * top_count)
    onehot = (chosen[:, None] == jnp.arange(experts, dtype=jnp.int32)).astype(jnp.float32)
    count = part_rows * top_count
    earlier = (jnp.arange(count)[:, None] > jnp.arange(count)[None, :]).astype(jnp.float32)
    rank = jnp.sum(jnp.dot(earlier, onehot) * onehot, axis=-1).astype(jnp.int32)
    slots = chosen * capacity + rank
    mine_hit = (slots[:, None] == jnp.arange(slot_count, dtype=jnp.int32)).astype(jnp.bfloat16)
    mine_hit = mine_hit.reshape(part_rows, top_count, slot_count)
    outgoing = jnp.einsum(
        "rs,rd->sd", jnp.sum(mine_hit, axis=1), own_rows, preferred_element_type=jnp.float32
    )
    outgoing = outgoing.astype(jnp.bfloat16).reshape(experts, capacity, model_dim)

    arrived, lat_all = spread(outgoing, lat_own, quarters)
    lat_rows = jnp.transpose(lat_all, (2, 1, 0, 3, 4)).reshape(n_ep * tok_rows, lat_own.shape[1])

    shape = arrived.shape
    gate = jnp.einsum("abecd,df->abecf", arrived, w_gate[0], preferred_element_type=jnp.float32)
    upward = jnp.einsum("abecd,df->abecf", arrived, w_up[0], preferred_element_type=jnp.float32)
    hidden = (jax.nn.silu(gate) * upward).astype(jnp.bfloat16)
    partial = jnp.einsum("abecf,fd->aebcd", hidden, w_down[0], preferred_element_type=jnp.float32)
    returned = collect(partial.astype(jnp.bfloat16))

    query = rms_norm(
        queries.astype(jnp.float32).reshape(tok_rows, head_count, nope_dim + rope_dim), query_gain
    )
    query_nope = query[..., :nope_dim].astype(jnp.bfloat16)
    query_rope = rotate(query[..., nope_dim:], rot_cos[:, None, :], rot_sin[:, None, :]).astype(
        jnp.bfloat16
    )
    attended = attend(
        lat_rows,
        w_key_up,
        w_value_up,
        jnp.transpose(query_nope, (1, 0, 2)),
        jnp.transpose(query_rope, (1, 0, 2)),
        key_gain,
        out_gain,
    )

    picked = jnp.einsum(
        "rks,sd->rkd",
        mine_hit,
        returned.reshape(slot_count, model_dim),
        preferred_element_type=jnp.float32,
    )
    own_weights = mine(route_weights, part_rows)
    moe_out = jnp.sum(picked * own_weights[:, :, None], axis=1).astype(jnp.bfloat16)
    return (attended, moe_out)


def solution(mesh):
    return jax.shard_map(
        on_device,
        mesh=mesh,
        in_specs=(
            P("ep", "tp"),
            P("ep", None),
            P("ep", None),
            P(),
            P(None, "tp"),
            P(None, "tp"),
            P(),
            P(),
            P(),
            P(),
            P("ep", None),
            P(),
            P("ep", None),
            P("ep", None),
            P("ep", None, "tp"),
            P("ep", None, "tp"),
            P("ep", "tp", None),
        ),
        out_specs=(P("ep", "tp"), P(("ep", "tp"), None)),
        check_vma=False,
    )
```

```python
import functools
import math

import jax
import jax.numpy as jnp
import numpy as np
from jax import lax
from jax.experimental import pallas as pl
from jax.experimental.pallas import tpu as pltpu
from jax.sharding import PartitionSpec as P

EPS = 1e-06
THETA = 500000.0


def rms_norm(values, norm_gain):
    return values * lax.rsqrt(jnp.mean(values * values, axis=-1, keepdims=True) + EPS) * norm_gain


def rope_tables(positions, rope_dim):
    freqs = 1.0 / THETA ** (jnp.arange(0, rope_dim, 2, dtype=jnp.float32) / rope_dim)
    angles = positions.astype(jnp.float32)[:, None] * freqs[None, :]
    return (jnp.cos(angles), jnp.sin(angles))


def rotate(values, rot_cos, rot_sin):
    half_dim = values.shape[-1] // 2
    first_half = values[..., :half_dim]
    second_half = values[..., half_dim:]
    return jnp.concatenate(
        [
            first_half * rot_cos - second_half * rot_sin,
            second_half * rot_cos + first_half * rot_sin,
        ],
        axis=-1,
    )

MESH = pl.DeviceIdType.MESH
VMEM = pltpu.VMEM


def remote(src, dst, send, recv, device):
    return pltpu.make_async_remote_copy(
        src_ref=src, dst_ref=dst, send_sem=send, recv_sem=recv, device_id=device, device_id_type=MESH
    )


def greet(me, quarter, n_ep, highs):
    high, low = quarter // 2, quarter % 2
    barrier = pltpu.get_barrier_semaphore()

    def hello(device):
        pl.semaphore_signal(barrier, inc=1, device_id=device, device_id_type=MESH)

    def hello_ep(step, carry):
        hello((lax.rem(me + step, n_ep), quarter))
        return carry

    lax.fori_loop(1, n_ep, hello_ep, 0)
    hello((me, high * 2 + 1 - low))
    for step in range(1, highs):
        hello((me, lax.rem(high + step, highs) * 2 + low))
    pl.semaphore_wait(barrier, n_ep - 1 + 1 + highs - 1)


def spread_kernel(
    n_ep, highs, rows_ref, lat_ref, arrived, lat_all,
    own_sem, ep_send, ep_recv, high_send, high_recv, low_send, low_recv,
):
    me, quarter = lax.axis_index("ep"), lax.axis_index("tp")
    high, low = quarter // 2, quarter % 2
    partner = (me, high * 2 + 1 - low)
    greet(me, quarter, n_ep, highs)
    payloads = (
        (lambda j: rows_ref.at[j], arrived),
        (lambda j: lat_ref, lat_all),
    )
    own = [
        pltpu.make_async_copy(outgoing(me), into.at[low, high, me], own_sem.at[p])
        for p, (outgoing, into) in enumerate(payloads)
    ]
    for copy in own:
        copy.start()

    def ep_copy(p, step):
        outgoing, into = payloads[p]
        j = lax.rem(me + step, n_ep)
        return remote(
            outgoing(j), into.at[low, high, me], ep_send.at[p, step], ep_recv.at[p, step], (j, quarter)
        )

    def ep_arrival(p, step):
        outgoing, into = payloads[p]
        j = lax.rem(me + n_ep - step, n_ep)
        return remote(
            outgoing(me), into.at[low, high, j], ep_send.at[p, step], ep_recv.at[p, step], (j, quarter)
        )

    def high_copy(p, step, hop):
        into = payloads[p][1]
        j = lax.rem(me + n_ep - step, n_ep)
        block = into.at[low, high, j]
        return remote(
            block, block, high_send.at[p, hop, step], high_recv.at[p, hop, step],
            (me, lax.rem(high + hop, highs) * 2 + low),
        )

    def high_arrival(p, step, hop):
        into = payloads[p][1]
        j = lax.rem(me + n_ep - step, n_ep)
        block = into.at[low, lax.rem(high + highs - hop, highs), j]
        return remote(
            block, block, high_send.at[p, hop, step], high_recv.at[p, hop, step],
            (me, lax.rem(high + hop, highs) * 2 + low),
        )

    def low_copy(p, step, hop, side):
        into = payloads[p][1]
        j = lax.rem(me + n_ep - step, n_ep)
        block = into.at[side, lax.rem(high + highs - hop, highs), j]
        return remote(block, block, low_send.at[p, hop, step], low_recv.at[p, hop, step], partner)

    def start_ep(step, carry, p):
        ep_copy(p, step).start()
        return carry

    def forward(step, carry, p):
        ep_arrival(p, step).wait_recv()
        for hop in range(1, highs):
            high_copy(p, step, hop).start()
        low_copy(p, step, 0, low).start()
        return carry

    def forward_low(step, carry, p):
        for hop in range(1, highs):
            high_arrival(p, step, hop).wait_recv()
            low_copy(p, step, hop, low).start()
        return carry

    def finish(step, carry, p):
        for hop in range(highs):
            low_copy(p, step, hop, 1 - low).wait_recv()
            low_copy(p, step, hop, low).wait_send()
        for hop in range(1, highs):
            high_copy(p, step, hop).wait_send()
        return carry

    def finish_ep(step, carry, p):
        ep_copy(p, step).wait_send()
        return carry

    for p in range(2):
        lax.fori_loop(1, n_ep, functools.partial(start_ep, p=p), 0)
    for p in range(2):
        own[p].wait()
        for hop in range(1, highs):
            high_copy(p, 0, hop).start()
        low_copy(p, 0, 0, low).start()
        lax.fori_loop(1, n_ep, functools.partial(forward, p=p), 0)
    for p in range(2):
        lax.fori_loop(0, n_ep, functools.partial(forward_low, p=p), 0)
    for p in range(2):
        lax.fori_loop(0, n_ep, functools.partial(finish, p=p), 0)
        lax.fori_loop(1, n_ep, functools.partial(finish_ep, p=p), 0)


def spread(rows, lat, quarters):
    n_ep, cap, model_dim = rows.shape
    highs = quarters // 2
    dma = pltpu.SemaphoreType.DMA
    return pl.pallas_call(
        functools.partial(spread_kernel, n_ep, highs),
        out_shape=(
            jax.ShapeDtypeStruct((2, highs, n_ep, cap, model_dim), rows.dtype),
            jax.ShapeDtypeStruct((2, highs, n_ep) + lat.shape, lat.dtype),
        ),
        in_specs=[pl.BlockSpec(memory_space=VMEM)] * 2,
        out_specs=(pl.BlockSpec(memory_space=VMEM),) * 2,
        scratch_shapes=[
            dma((2,)),
            dma((2, n_ep)),
            dma((2, n_ep)),
            dma((2, highs, n_ep)),
            dma((2, highs, n_ep)),
            dma((2, highs, n_ep)),
            dma((2, highs, n_ep)),
        ],
        compiler_params=pltpu.CompilerParams(
            collective_id=0, has_side_effects=True, vmem_limit_bytes=60 << 20
        ),
        name="spread",
    )(rows, lat)


def collect_kernel(
    n_ep, highs, part_ref, ret, low_buf, high_buf, sum_buf, final_buf,
    low_send, low_recv, high_send, high_recv, ep_send, ep_recv,
):
    me, quarter = lax.axis_index("ep"), lax.axis_index("tp")
    high, low = quarter // 2, quarter % 2
    partner = (me, high * 2 + 1 - low)
    greet(me, quarter, n_ep, highs)

    def low_copy(step):
        j = lax.rem(me + step, n_ep)
        return remote(
            part_ref.at[1 - low, j], low_buf.at[j], low_send.at[step], low_recv.at[step], partner
        )

    def high_copy(step, hop):
        j = lax.rem(me + step, n_ep)
        other = lax.rem(high + hop, highs)
        return remote(
            sum_buf.at[j, other], high_buf.at[hop, j], high_send.at[hop, step],
            high_recv.at[hop, step], (me, other * 2 + low),
        )

    def ep_copy(step):
        j = lax.rem(me + step, n_ep)
        return remote(final_buf.at[j], ret.at[me], ep_send.at[step], ep_recv.at[step], (j, quarter))

    def ep_arrival(step):
        j = lax.rem(me + n_ep - step, n_ep)
        return remote(final_buf.at[j], ret.at[j], ep_send.at[step], ep_recv.at[step], (j, quarter))

    def start_low(step, carry):
        low_copy(step).start()
        return carry

    def add_low(step, carry):
        low_copy(step).wait_recv()
        j = lax.rem(me + step, n_ep)
        sum_buf[j] = (
            part_ref[low, j].astype(jnp.float32) + low_buf[j].astype(jnp.float32)
        ).astype(jnp.bfloat16)
        for hop in range(1, highs):
            high_copy(step, hop).start()
        return carry

    def total(step):
        j = lax.rem(me + step, n_ep)
        value = part_ref[low, j, high].astype(jnp.float32) + low_buf[j, high].astype(jnp.float32)
        for hop in range(1, highs):
            high_copy(step, hop).wait_recv()
            value = value + high_buf[hop, j].astype(jnp.float32)
        return value.astype(jnp.bfloat16)

    def add_high(step, carry):
        final_buf[lax.rem(me + step, n_ep)] = total(step)
        ep_copy(step).start()
        return carry

    def finish(step, carry):
        ep_arrival(step).wait_recv()
        ep_copy(step).wait_send()
        return carry

    def finish_tp(step, carry):
        low_copy(step).wait_send()
        for hop in range(1, highs):
            high_copy(step, hop).wait_send()
        return carry

    lax.fori_loop(1, n_ep, start_low, 0)
    low_copy(0).start()
    lax.fori_loop(1, n_ep, add_low, 0)
    add_low(0, 0)
    lax.fori_loop(1, n_ep, add_high, 0)
    ret[me] = total(0)
    lax.fori_loop(1, n_ep, finish, 0)
    lax.fori_loop(0, n_ep, finish_tp, 0)


def collect(partial):
    _, n_ep, highs, cap, model_dim = partial.shape
    dma = pltpu.SemaphoreType.DMA
    kind = partial.dtype
    return pl.pallas_call(
        functools.partial(collect_kernel, n_ep, highs),
        out_shape=jax.ShapeDtypeStruct((n_ep, cap, model_dim), kind),
        in_specs=[pl.BlockSpec(memory_space=VMEM)],
        out_specs=pl.BlockSpec(memory_space=VMEM),
        scratch_shapes=[
            VMEM((n_ep, highs, cap, model_dim), kind),
            VMEM((highs, n_ep, cap, model_dim), kind),
            VMEM((n_ep, highs, cap, model_dim), kind),
            VMEM((n_ep, cap, model_dim), kind),
            dma((n_ep,)),
            dma((n_ep,)),
            dma((highs, n_ep)),
            dma((highs, n_ep)),
            dma((n_ep,)),
            dma((n_ep,)),
        ],
        compiler_params=pltpu.CompilerParams(
            collective_id=1, has_side_effects=True, vmem_limit_bytes=62 << 20
        ),
        name="collect",
    )(partial)


def attend_kernel(
    heads, nope_dim, value_dim, latent_dim, scale,
    lat_ref, wk_ref, wv_ref, qn_ref, qr_ref, kg_ref, og_ref, out_ref, acc, den,
):
    block = pl.program_id(0)
    block_rows = lat_ref.shape[0]
    tok_rows = qn_ref.shape[1]
    offset = lax.axis_index("ep") * tok_rows
    first = block * block_rows

    @pl.when(block == 0)
    def _():
        acc[...] = jnp.zeros_like(acc)
        den[...] = jnp.zeros_like(den)

    @pl.when(first <= offset + tok_rows - 1)
    def _():
        latent = lat_ref[:, :latent_dim]
        rot_key = lat_ref[:, latent_dim:]
        keys = jnp.dot(latent, wk_ref[...], preferred_element_type=jnp.float32)
        values = jnp.dot(latent, wv_ref[...], preferred_element_type=jnp.float32).astype(jnp.bfloat16)
        shape = (tok_rows, block_rows)
        visible = offset + lax.broadcasted_iota(jnp.int32, shape, 0) >= first + lax.broadcasted_iota(
            jnp.int32, shape, 1
        )
        across = (((1,), (1,)), ((), ()))
        for head in range(heads):
            key = keys[:, head * nope_dim : (head + 1) * nope_dim]
            key = rms_norm(key, kg_ref[...]).astype(jnp.bfloat16)
            scores = lax.dot_general(qn_ref[head], key, across, preferred_element_type=jnp.float32)
            scores = scores + lax.dot_general(
                qr_ref[head], rot_key, across, preferred_element_type=jnp.float32
            )
            weights = jnp.where(visible, jnp.exp(scores * scale), 0.0)
            den[head] += jnp.sum(weights, axis=-1, keepdims=True)
            acc[head] += jnp.dot(
                weights.astype(jnp.bfloat16),
                values[:, head * value_dim : (head + 1) * value_dim],
                preferred_element_type=jnp.float32,
            )

    @pl.when(block == pl.num_programs(0) - 1)
    def _():
        for head in range(heads):
            mixed = rms_norm(acc[head] / den[head], og_ref[...])
            out_ref[:, head * value_dim : (head + 1) * value_dim] = mixed.astype(jnp.bfloat16)


def attend(lat_rows, w_key_up, w_value_up, query_nope, query_rope, key_gain, out_gain):
    heads, tok_rows, nope_dim = query_nope.shape
    rope_dim = query_rope.shape[2]
    value_dim = out_gain.shape[0]
    total, width = lat_rows.shape
    block_rows = math.gcd(total, 512)
    whole = pl.BlockSpec(memory_space=VMEM)
    return pl.pallas_call(
        functools.partial(
            attend_kernel, heads, nope_dim, value_dim, width - rope_dim, (nope_dim + rope_dim) ** (-0.5)
        ),
        grid=(total // block_rows,),
        out_shape=jax.ShapeDtypeStruct((tok_rows, heads * value_dim), jnp.bfloat16),
        in_specs=[pl.BlockSpec((block_rows, width), lambda b: (b, 0))] + [whole] * 6,
        out_specs=pl.BlockSpec((tok_rows, heads * value_dim), lambda b: (0, 0)),
        scratch_shapes=[
            VMEM((heads, tok_rows, value_dim), jnp.float32),
            VMEM((heads, tok_rows, 1), jnp.float32),
        ],
        name="attend",
    )(
        lat_rows, w_key_up, w_value_up, query_nope, query_rope,
        key_gain.reshape(1, -1), out_gain.reshape(1, -1),
    )


LANES = 128
TILE = 256


def layer_kernel(
    n_ep, heads, nope_dim, rope_dim, value_dim,
    tok_hbm, mg_hbm, routes_hbm, rw_hbm, kv_hbm, rk_hbm, freq_hbm, lg_hbm, rg_hbm, q_hbm, qg_hbm,
    wk_hbm, wv_hbm, kg_hbm, og_hbm, wg_hbm, wu_hbm, wd_hbm,
    att_ref, moe_ref,
    tok_ref, mg_ref, routes_ref, rw_ref, kv_ref, rk_ref, freq_ref, lg_ref, rg_ref, q_ref, qg_ref,
    wk_ref, wv_ref, kg_ref, og_ref,
    wgu, wd, normed, rows_out, arrived, hid, part, low_buf, sum_buf, high_buf, final_buf, ret, hits,
    lat_all, cos_ref, sin_ref, qn, qr, acc, den,
    in_sem, w_sem, ep_send, ep_recv, high_send, high_recv, low_send, low_recv,
    rlow_send, rlow_recv, rhigh_send, rhigh_recv, rep_send, rep_recv,
    lz_send, lz_recv, ly_send, ly_recv, ll_send, ll_recv,
):
    me, quarter = lax.axis_index("ep"), lax.axis_index("tp")
    n_z = n_ep // 2
    z, y = me // 2, lax.rem(me, 2)
    high, low = quarter // 2, lax.rem(quarter, 2)
    partner = (me, high * 2 + 1 - low)
    across = (me, (1 - high) * 2 + low)
    bf16, f32 = jnp.bfloat16, jnp.float32
    cap = rows_out.shape[1]
    model_dim = rows_out.shape[2]
    tok_rows = tok_ref.shape[0]
    part_rows = tok_rows // 4
    ff = wd.shape[0]
    half = tok_rows // 2
    barrier = pltpu.get_barrier_semaphore()

    def hello(device):
        pl.semaphore_signal(barrier, inc=1, device_id=device, device_id_type=MESH)

    def hello_ep(step, carry):
        hello((lax.rem(me + step, n_ep), quarter))
        return carry

    lax.fori_loop(1, n_ep, hello_ep, 0)
    hello(partner)
    hello(across)

    def weight_copies():
        out = []
        for i in range(ff // LANES):
            out.append((wg_hbm.at[0, :, pl.ds(LANES * i, LANES)], wgu.at[:, pl.ds(TILE * i, LANES)]))
            out.append((wu_hbm.at[0, :, pl.ds(LANES * i, LANES)], wgu.at[:, pl.ds(TILE * i + LANES, LANES)]))
        out.append((wd_hbm.at[0], wd))
        return [pltpu.make_async_copy(a, b, w_sem.at[i]) for i, (a, b) in enumerate(out)]

    sources = (
        tok_hbm, mg_hbm, routes_hbm, rw_hbm, kv_hbm, rk_hbm, freq_hbm, lg_hbm, rg_hbm, q_hbm, qg_hbm,
        wk_hbm, wv_hbm, kg_hbm, og_hbm,
    )
    loaded = (
        tok_ref, mg_ref, routes_ref, rw_ref, kv_ref, rk_ref, freq_ref, lg_ref, rg_ref, q_ref, qg_ref,
        wk_ref, wv_ref, kg_ref, og_ref,
    )
    loads = [
        pltpu.make_async_copy(source, into, in_sem.at[i])
        for i, (source, into) in enumerate(zip(sources, loaded))
    ]
    for copy in loads:
        copy.start()
    for copy in weight_copies():
        copy.start()

    def ep_to(s, t):
        return lax.rem(z + s, n_z) * 2 + lax.rem(y + t, 2)

    def ep_from(s, t):
        return lax.rem(z + n_z - s, n_z) * 2 + lax.rem(y + t, 2)


    tokens = (1, tok_rows)
    token = lax.broadcasted_iota(jnp.int32, tokens, 1)

    def quarter_of(index):
        return sum((index >= q * part_rows).astype(jnp.int32) for q in range(1, 4))

    def hit_matrix(count, places):
        slot = lax.broadcasted_iota(jnp.int32, (count, places[0].shape[1]), 0).astype(f32)
        return sum((slot == place).astype(f32) for place in places)

    def gather_rows(select, into):
        select = select.astype(bf16)
        wide = 512
        for n in range(model_dim // wide):
            cols = slice(n * wide, (n + 1) * wide)
            rows = jnp.dot(select, normed[:, cols], preferred_element_type=f32).astype(bf16)
            into(cols, rows, wide)

    def own_part(row):
        return sum(
            jnp.where(quarter == q, row[:, q * part_rows : (q + 1) * part_rows], 0.0) for q in range(4)
        )

    def ranks():
        shape = (tok_rows, tok_rows)
        before, after = lax.broadcasted_iota(jnp.int32, shape, 0), lax.broadcasted_iota(jnp.int32, shape, 1)
        earlier = ((before < after) & (quarter_of(before) == quarter_of(after))).astype(bf16)
        experts = lax.broadcasted_iota(jnp.int32, (n_ep, tok_rows), 0)
        ones = [(routes_ref[k : k + 1, :] == experts).astype(f32) for k in range(2)]
        rank = jnp.dot((ones[0] + ones[1]).astype(bf16), earlier, preferred_element_type=f32)
        return [jnp.sum(rank * one, axis=0, keepdims=True) for one in ones]

    def norm_tokens():
        step = 64
        for i in range(tok_rows // step):
            rows = tok_ref[i * step : (i + 1) * step, :].astype(f32)
            normed[i * step : (i + 1) * step, :] = rms_norm(rows, mg_ref[...]).astype(bf16)

    def dispatch(rank):
        mine = quarter_of(token) == quarter
        places = [
            jnp.where(mine, routes_ref[k : k + 1, :].astype(f32) * cap + rank[k], -1.0) for k in range(2)
        ]

        def into(cols, rows, wide):
            rows_out[:, :, cols] = rows.reshape(n_ep, cap, wide)

        gather_rows(hit_matrix(n_ep * cap, places), into)

    def own_dispatch(rank):
        number = quarter_of(token)
        position = lax.rem(number, 2) * 2 + number // 2
        places = [
            jnp.where(routes_ref[k : k + 1, :] == me, position.astype(f32) * cap + rank[k], -1.0)
            for k in range(2)
        ]

        def into(cols, rows, wide):
            arrived[me, :, :, :, cols] = rows.reshape(2, 2, cap, wide)

        gather_rows(hit_matrix(4 * cap, places), into)

    def combine_matrices(rank):
        slot = lax.broadcasted_iota(jnp.int32, (n_ep * cap, part_rows), 0).astype(f32)
        weighted = jnp.zeros((n_ep * cap, part_rows), f32)
        for k in range(2):
            place = own_part(routes_ref[k : k + 1, :].astype(f32) * cap + rank[k])
            weighted += jnp.where(slot == place, own_part(rw_ref[k : k + 1, :]), 0.0)
        upper = weighted.astype(bf16)
        hits[0] = upper
        hits[1] = (weighted - upper.astype(f32)).astype(bf16)

    for copy in loads[:4]:
        copy.wait()
    rank = ranks()
    norm_tokens()
    dispatch(rank)
    pl.semaphore_wait(barrier, n_ep + 1)

    def ep_copy(s, t):
        return remote(
            rows_out.at[ep_to(s, t)], arrived.at[me, low, high], ep_send.at[s, t], ep_recv.at[s, t],
            (ep_to(s, t), quarter),
        )

    def ep_arrival(s, t):
        j = ep_from(s, t)
        return remote(
            rows_out.at[j], arrived.at[j, low, high], ep_send.at[s, t], ep_recv.at[s, t], (j, quarter)
        )

    def high_copy(s, t, side):
        block = arrived.at[ep_from(s, t), low, side]
        return remote(block, block, high_send.at[s, t], high_recv.at[s, t], across)

    def low_copy(s, t, hop, side, core):
        block = arrived.at[ep_from(s, t), core, side]
        return remote(block, block, low_send.at[hop, s, t], low_recv.at[hop, s, t], partner)

    def each(s, body):
        for t in range(2):
            if t == 0:
                pl.when(s > 0)(functools.partial(body, s, 0))
            else:
                body(s, 1)

    def start_ep(s, carry):
        each(s, lambda s, t: ep_copy(s, t).start())
        return carry

    def order(i):
        if n_z % 2:
            return i
        return jnp.where(i < n_z - 1, lax.rem(2 * i, n_z - 1), n_z - 1)

    def send_rows(i):
        if i < n_z:
            start_ep(order(i), 0)

    start_ep(0, 0)
    send_rows(1)


    def lat_copy_z(k):
        block = lat_all.at[k, y, low]
        return remote(
            block, block, lz_send.at[k], lz_recv.at[k], (lax.rem(z + 1, n_z) * 2 + y, quarter)
        )

    def lat_copy_y(k, side):
        block = lat_all.at[k, side, low]
        return remote(block, block, ly_send.at[k], ly_recv.at[k], (z * 2 + 1 - y, quarter))

    def lat_copy_low(k, hop, core):
        block = lat_all.at[k, y if hop == 0 else 1 - y, core]
        return remote(block, block, ll_send.at[hop, k], ll_recv.at[hop, k], partner)

    def tables():
        half_dim = rope_dim // 2
        places = lax.broadcasted_iota(jnp.int32, (tok_rows, half_dim), 0) + me * tok_rows
        angles = places.astype(f32) * freq_ref[...]
        cos_ref[...] = jnp.cos(angles)
        sin_ref[...] = jnp.sin(angles)

    def lat_own():
        latent = rms_norm(kv_ref[...].astype(f32), lg_ref[...]).astype(bf16)
        raw = jnp.transpose(rk_ref[...].astype(f32))
        rot = rotate(rms_norm(raw, rg_ref[...]), cos_ref[...], sin_ref[...]).astype(bf16)
        step = lat_all.shape[3] - half
        for core in range(2):
            lat_all[z, y, core, :half] = latent[core * half : (core + 1) * half]
            first = core * half
            lat_all[z, y, core, half:] = jnp.concatenate(
                [rot[first + i : first + i + step] for i in range(0, half, step)], axis=1
            )

    def lat_send():
        pl.when(z < n_z - 1)(lambda: lat_copy_z(z).start())
        pl.when(y == 0)(lambda: lat_copy_y(z, y).start())

    def lat_step(k, carry):
        origin = z - k

        @pl.when(origin >= 0)
        def _():
            lat_copy_z(origin).wait_recv()
            pl.when(z < n_z - 1)(lambda: lat_copy_z(origin).start())
            lat_copy_y(origin, y).start()
            lat_copy_low(origin, 0, low).start()

        return carry

    def lat_side(k, carry):
        origin = z - k

        @pl.when((origin >= 0) & (k + y > 0))
        def _():
            lat_copy_y(origin, 1 - y).wait_recv()
            lat_copy_low(origin, 1, low).start()

        return carry


    def queries():
        raw = q_ref[...].astype(f32)
        width = nope_dim + rope_dim
        for head in range(heads):
            query = rms_norm(raw[:, head * width : (head + 1) * width], qg_ref[...])
            qn[head] = query[:, :nope_dim].astype(bf16)
            qr[head] = rotate(query[:, nope_dim:], cos_ref[...], sin_ref[...]).astype(bf16)

    scale = (nope_dim + rope_dim) ** (-0.5)

    def attend_block(zj, yj, own):
        latent = lat_all[zj, yj, :, :half].reshape(tok_rows, lat_all.shape[-1])
        rot_key = jnp.concatenate(
            [
                lat_all[zj, yj, core, half:, i : i + rope_dim]
                for core in range(2)
                for i in range(0, lat_all.shape[-1], rope_dim)
            ],
            axis=0,
        )
        keys = jnp.dot(latent, wk_ref[...], preferred_element_type=f32)
        values = jnp.dot(latent, wv_ref[...], preferred_element_type=f32).astype(bf16)
        lined = (((1,), (1,)), ((), ()))
        for head in range(heads):
            key = rms_norm(keys[:, head * nope_dim : (head + 1) * nope_dim], kg_ref[...]).astype(bf16)
            scores = lax.dot_general(qn[head], key, lined, preferred_element_type=f32)
            scores = scores + lax.dot_general(qr[head], rot_key, lined, preferred_element_type=f32)
            weights = jnp.exp(scores * scale)
            if own:
                shape = (tok_rows, tok_rows)
                visible = lax.broadcasted_iota(jnp.int32, shape, 0) >= lax.broadcasted_iota(jnp.int32, shape, 1)
                weights = jnp.where(visible, weights, 0.0)
            total = jnp.sum(weights, axis=-1, keepdims=True)
            mixed = jnp.dot(
                weights.astype(bf16), values[:, head * value_dim : (head + 1) * value_dim],
                preferred_element_type=f32,
            )
            if own:
                den[head] = total
                acc[head] = mixed
            else:
                den[head] += total
                acc[head] += mixed

    def attend_side(k):
        @pl.when((z >= k) & (k + y > 0))
        def _():
            lat_copy_low(z - k, 1, 1 - low).wait_recv()
            attend_block(z - k, 1 - y, False)

    def attend_line(k):
        @pl.when(z >= k)
        def _():
            lat_copy_low(z - k, 0, 1 - low).wait_recv()
            attend_block(z - k, y, False)


    def forward(s, t):
        ep_arrival(s, t).wait_recv()
        high_copy(s, t, high).start()
        low_copy(s, t, 0, high, low).start()

    def forward_low(s, t):
        high_copy(s, t, 1 - high).wait_recv()
        low_copy(s, t, 1, 1 - high, low).start()

    def arrive(s, t):
        low_copy(s, t, 0, high, 1 - low).wait_recv()
        low_copy(s, t, 1, 1 - high, 1 - low).wait_recv()

    def expert_up(s):
        first = lax.rem(z + n_z - s, n_z) * 2
        rows = arrived[pl.ds(first, 2)].reshape(8 * cap, model_dim)
        for i in range(ff // LANES):
            both = jnp.dot(rows, wgu[:, TILE * i : TILE * (i + 1)], preferred_element_type=f32)
            gate, upward = both[:, :LANES], both[:, LANES:]
            hid[:, LANES * i : LANES * (i + 1)] = (jax.nn.silu(gate) * upward).astype(bf16)

    def expert_down(s):
        first = lax.rem(z + n_z - s, n_z) * 2
        for n in range(model_dim // TILE):
            down = jnp.dot(hid[...], wd[:, TILE * n : TILE * (n + 1)], preferred_element_type=f32)
            part[pl.ds(first, 2), :, :, :, TILE * n : TILE * (n + 1)] = down.astype(bf16).reshape(
                2, 2, 2, cap, TILE
            )

    def rlow_copy(s, t):
        j = ep_from(s, t)
        return remote(part.at[j, 1 - low], low_buf.at[j], rlow_send.at[s, t], rlow_recv.at[s, t], partner)

    def rhigh_copy(s, t):
        j = ep_from(s, t)
        return remote(sum_buf.at[j], high_buf.at[j], rhigh_send.at[s, t], rhigh_recv.at[s, t], across)

    def rep_copy(s, t):
        j = ep_from(s, t)
        return remote(final_buf.at[j], ret.at[me], rep_send.at[s, t], rep_recv.at[s, t], (j, quarter))

    def rep_arrival(s, t):
        j = ep_to(s, t)
        return remote(final_buf.at[j], ret.at[j], rep_send.at[s, t], rep_recv.at[s, t], (j, quarter))

    def reduce_low(s, t):
        j = ep_from(s, t)
        rlow_copy(s, t).wait_recv()
        sum_buf[j] = (part[j, low, 1 - high].astype(f32) + low_buf[j, 1 - high].astype(f32)).astype(bf16)
        rhigh_copy(s, t).start()

    def reduce_high(s, t):
        j = ep_from(s, t)
        rhigh_copy(s, t).wait_recv()
        value = part[j, low, high].astype(f32) + low_buf[j, high].astype(f32) + high_buf[j].astype(f32)
        if isinstance(s, int) and s + t == 0:
            ret[me] = value.astype(bf16)
        else:
            final_buf[j] = value.astype(bf16)
            rep_copy(s, t).start()

    def both(body, s):
        body(s, 0)
        body(s, 1)

    def lat_hop(k):
        if k < n_z:
            lat_step(k, 0)

    def attend_step(k):
        if k < n_z:
            if k > 0:
                attend_line(k)
            attend_side(k)

    own_dispatch(rank)
    combine_matrices(rank)
    for copy in loads[4:]:
        copy.wait()
    tables()
    forward(0, 1)
    lat_own()
    queries()
    attend_block(z, y, True)

    before, between, after = {}, {}, {}

    def at(table, i, body, *args):
        table.setdefault(i, []).append(functools.partial(body, *args))

    def weights_here():
        for copy in weight_copies():
            copy.wait()

    last = n_z - 1
    at(before, 0, weights_here)
    at(before, 0, send_rows, 2)
    at(between, 0, lambda: both(forward, order(1)))
    for i in range(3, n_z):
        at(after, 0, send_rows, i)
    at(after, 0, lambda: both(forward, order(2)))
    at(before, 1, lat_send)
    for i in range(1, last):
        if i + 2 <= last:
            at(between, i, lambda i=i: both(forward, order(i + 2)))
        if i == last - 1:
            at(after, i, lat_hop, 1)
        at(after, i, lambda i=i: both(reduce_low, order(i)))

    def run(table, i):
        for place, bodies in table.items():

            @pl.when(i == place)
            def _():
                for body in bodies:
                    body()

    def stage(i, carry):
        s = order(i)
        each(s, forward_low)
        each(s, arrive)
        run(before, i)
        expert_up(s)
        run(between, i)
        expert_down(s)
        for t in range(2):
            rlow_copy(s, t).start()
        run(after, i)
        return carry

    lax.fori_loop(0, n_z, stage, 0)
    for i in range(1, last - 1):
        both(reduce_high, order(i))
    both(reduce_low, order(last))
    both(reduce_low, 0)
    lat_hop(2)
    lat_side(0, 0)
    attend_step(0)
    both(reduce_high, order(last - 1))
    lat_side(1, 0)
    attend_step(1)
    for far in range(3, n_z):
        lat_hop(far)
    both(reduce_high, order(last))
    lat_side(2, 0)
    attend_step(2)
    reduce_high(0, 1)
    reduce_high(0, 0)
    for k in range(3, n_z):
        lat_side(k, 0)
        attend_step(k)
    for head in range(heads):
        mixed = rms_norm(acc[head] / den[head], og_ref[...])
        att_ref[:, head * value_dim : (head + 1) * value_dim] = mixed.astype(bf16)

    def returned(s, carry):
        each(s, lambda s, t: rep_arrival(s, t).wait_recv())
        return carry

    lax.fori_loop(0, n_z, returned, 0)
    wide = 512
    lined = (((0,), (0,)), ((), ()))
    for n in range(model_dim // wide):
        values = ret[:, :, n * wide : (n + 1) * wide].reshape(n_ep * cap, wide)
        mixed = lax.dot_general(hits[0], values, lined, preferred_element_type=f32)
        mixed += lax.dot_general(hits[1], values, lined, preferred_element_type=f32)
        moe_ref[:, n * wide : (n + 1) * wide] = mixed.astype(bf16)

    def sent(s, carry):
        def rows_sent(s, t):
            ep_copy(s, t).wait_send()
            high_copy(s, t, high).wait_send()
            low_copy(s, t, 0, high, low).wait_send()
            low_copy(s, t, 1, 1 - high, low).wait_send()
            rep_copy(s, t).wait_send()

        each(s, rows_sent)
        for t in range(2):
            rlow_copy(s, t).wait_send()
            rhigh_copy(s, t).wait_send()

        origin = z - s

        @pl.when(origin >= 0)
        def _():
            pl.when(z < n_z - 1)(lambda: lat_copy_z(origin).wait_send())
            pl.when((s > 0) | (y == 0))(lambda: lat_copy_y(origin, y).wait_send())
            pl.when(s > 0)(lambda: lat_copy_low(origin, 0, low).wait_send())
            pl.when(s + y > 0)(lambda: lat_copy_low(origin, 1, low).wait_send())

        return carry

    lax.fori_loop(0, n_z, sent, 0)


def layer(
    queries, kv_latent, rope_key, latent_gain, w_key_up, w_value_up, query_gain, key_gain,
    rope_gain, out_gain, moe_tokens, moe_gain, routes, route_weights, w_gate, w_up, w_down, n_ep, cap,
):
    tok_rows = queries.shape[0]
    nope_dim, rope_dim, value_dim = key_gain.shape[0], rope_key.shape[1], out_gain.shape[0]
    heads = w_key_up.shape[1] // nope_dim
    model_dim = moe_tokens.shape[1]
    part_rows = tok_rows // 4
    ff = w_down.shape[1]
    n_z = n_ep // 2
    packed = tok_rows // 2 * rope_dim // kv_latent.shape[1]
    dma = pltpu.SemaphoreType.DMA
    kind, f32 = jnp.bfloat16, jnp.float32
    pairs = (n_z, 2)
    block = (cap, model_dim)
    freqs = (1.0 / THETA ** (np.arange(0, rope_dim, 2) / rope_dim)).astype(np.float32)
    small = (
        moe_tokens, moe_gain.reshape(1, -1), routes.T, route_weights.T, kv_latent, rope_key.T,
        freqs.reshape(1, -1), latent_gain.reshape(1, -1), rope_gain.reshape(1, -1), queries,
        query_gain.reshape(1, -1), w_key_up, w_value_up, key_gain.reshape(1, -1), out_gain.reshape(1, -1),
    )
    return pl.pallas_call(
        functools.partial(layer_kernel, n_ep, heads, nope_dim, rope_dim, value_dim),
        out_shape=(
            VMEM((tok_rows, heads * value_dim), kind),
            VMEM((part_rows, model_dim), kind),
        ),
        in_specs=[pl.BlockSpec(memory_space=pltpu.HBM)] * (len(small) + 3),
        out_specs=(pl.BlockSpec(memory_space=VMEM),) * 2,
        scratch_shapes=[VMEM(array.shape, array.dtype) for array in small] + [
            VMEM((model_dim, 2 * ff), kind),
            VMEM((ff, model_dim), kind),
            VMEM((tok_rows, model_dim), kind),
            VMEM((n_ep,) + block, kind),
            VMEM((n_ep, 2, 2) + block, kind),
            VMEM((8 * cap, ff), kind),
            VMEM((n_ep, 2, 2) + block, kind),
            VMEM((n_ep, 2) + block, kind),
            VMEM((n_ep,) + block, kind),
            VMEM((n_ep,) + block, kind),
            VMEM((n_ep,) + block, kind),
            VMEM((n_ep,) + block, kind),
            VMEM((2, n_ep * cap, part_rows), kind),
            VMEM((n_z, 2, 2, tok_rows // 2 + packed, kv_latent.shape[1]), kind),
            VMEM((tok_rows, rope_dim // 2), f32),
            VMEM((tok_rows, rope_dim // 2), f32),
            VMEM((heads, tok_rows, nope_dim), kind),
            VMEM((heads, tok_rows, rope_dim), kind),
            VMEM((heads, tok_rows, value_dim), f32),
            VMEM((heads, tok_rows, 1), f32),
            dma((len(small),)),
            dma((2 * (ff // LANES) + 1,)),
            dma(pairs), dma(pairs), dma(pairs), dma(pairs), dma((2,) + pairs), dma((2,) + pairs),
            dma(pairs), dma(pairs), dma(pairs), dma(pairs), dma(pairs), dma(pairs),
            dma((n_z,)), dma((n_z,)), dma((n_z,)), dma((n_z,)), dma((2, n_z)), dma((2, n_z)),
        ],
        compiler_params=pltpu.CompilerParams(
            collective_id=2, has_side_effects=True, vmem_limit_bytes=62 << 20
        ),
        name="layer",
    )(*small, w_gate, w_up, w_down)


def on_device(
    queries,
    kv_latent,
    rope_key,
    latent_gain,
    w_key_up,
    w_value_up,
    query_gain,
    key_gain,
    rope_gain,
    out_gain,
    moe_tokens,
    moe_gain,
    routes,
    route_weights,
    w_gate,
    w_up,
    w_down,
):
    quarters = lax.axis_size("tp")
    n_ep = lax.axis_size("ep")
    my_part = lax.axis_index("tp")
    tok_rows = queries.shape[0]
    nope_dim = key_gain.shape[0]
    value_dim = out_gain.shape[0]
    rope_dim = rope_key.shape[1]
    head_count = w_key_up.shape[1] // nope_dim
    positions = lax.axis_index("ep") * tok_rows + jnp.arange(tok_rows, dtype=jnp.int32)
    rot_cos, rot_sin = rope_tables(positions, rope_dim)
    n_rows, model_dim = moe_tokens.shape
    top_count = routes.shape[1]
    part_rows = n_rows // quarters
    experts = n_ep * w_gate.shape[0]
    capacity = (3 * top_count * part_rows + 2 * experts - 1) // (2 * experts)
    one_kernel = quarters == 4 and n_ep % 2 == 0 and w_gate.shape[0] == 1 and top_count == 2
    lat_parts = kv_latent.shape[1] // rope_dim
    one_kernel = one_kernel and n_ep >= 8 and kv_latent.shape[1] % LANES == 0
    one_kernel = one_kernel and kv_latent.shape[1] % rope_dim == 0 and n_rows % (32 * lat_parts) == 0
    if one_kernel and capacity % 8 == 0 and w_down.shape[1] % LANES == 0 and model_dim % 512 == 0:
        return layer(
            queries, kv_latent, rope_key, latent_gain, w_key_up, w_value_up, query_gain, key_gain, rope_gain,
            out_gain, moe_tokens, moe_gain, routes, route_weights, w_gate, w_up, w_down, n_ep, capacity,
        )
    lat_part = tok_rows // quarters

    def mine(values, rows):
        return lax.dynamic_slice_in_dim(values, my_part * rows, rows, 0)

    latent = rms_norm(mine(kv_latent, lat_part).astype(jnp.float32), latent_gain)
    rot_key = rotate(
        rms_norm(mine(rope_key, lat_part).astype(jnp.float32), rope_gain),
        mine(rot_cos, lat_part),
        mine(rot_sin, lat_part),
    )
    lat_own = jnp.concatenate([latent.astype(jnp.bfloat16), rot_key.astype(jnp.bfloat16)], axis=1)

    slot_count = experts * capacity
    own_rows = rms_norm(mine(moe_tokens, part_rows).astype(jnp.float32), moe_gain).astype(jnp.bfloat16)
    chosen = mine(routes, part_rows).reshape(part_rows * top_count)
    onehot = (chosen[:, None] == jnp.arange(experts, dtype=jnp.int32)).astype(jnp.float32)
    count = part_rows * top_count
    earlier = (jnp.arange(count)[:, None] > jnp.arange(count)[None, :]).astype(jnp.float32)
    rank = jnp.sum(jnp.dot(earlier, onehot) * onehot, axis=-1).astype(jnp.int32)
    slots = chosen * capacity + rank
    mine_hit = (slots[:, None] == jnp.arange(slot_count, dtype=jnp.int32)).astype(jnp.bfloat16)
    mine_hit = mine_hit.reshape(part_rows, top_count, slot_count)
    outgoing = jnp.einsum(
        "rs,rd->sd", jnp.sum(mine_hit, axis=1), own_rows, preferred_element_type=jnp.float32
    )
    outgoing = outgoing.astype(jnp.bfloat16).reshape(experts, capacity, model_dim)

    arrived, lat_all = spread(outgoing, lat_own, quarters)
    lat_rows = jnp.transpose(lat_all, (2, 1, 0, 3, 4)).reshape(n_ep * tok_rows, lat_own.shape[1])

    shape = arrived.shape
    gate = jnp.einsum("abecd,df->abecf", arrived, w_gate[0], preferred_element_type=jnp.float32)
    upward = jnp.einsum("abecd,df->abecf", arrived, w_up[0], preferred_element_type=jnp.float32)
    hidden = (jax.nn.silu(gate) * upward).astype(jnp.bfloat16)
    partial = jnp.einsum("abecf,fd->aebcd", hidden, w_down[0], preferred_element_type=jnp.float32)
    returned = collect(partial.astype(jnp.bfloat16))

    query = rms_norm(
        queries.astype(jnp.float32).reshape(tok_rows, head_count, nope_dim + rope_dim), query_gain
    )
    query_nope = query[..., :nope_dim].astype(jnp.bfloat16)
    query_rope = rotate(query[..., nope_dim:], rot_cos[:, None, :], rot_sin[:, None, :]).astype(
        jnp.bfloat16
    )
    attended = attend(
        lat_rows,
        w_key_up,
        w_value_up,
        jnp.transpose(query_nope, (1, 0, 2)),
        jnp.transpose(query_rope, (1, 0, 2)),
        key_gain,
        out_gain,
    )

    picked = jnp.einsum(
        "rks,sd->rkd",
        mine_hit,
        returned.reshape(slot_count, model_dim),
        preferred_element_type=jnp.float32,
    )
    own_weights = mine(route_weights, part_rows)
    moe_out = jnp.sum(picked * own_weights[:, :, None], axis=1).astype(jnp.bfloat16)
    return (attended, moe_out)


def solution(mesh):
    return jax.shard_map(
        on_device,
        mesh=mesh,
        in_specs=(
            P("ep", "tp"),
            P("ep", None),
            P("ep", None),
            P(),
            P(None, "tp"),
            P(None, "tp"),
            P(),
            P(),
            P(),
            P(),
            P("ep", None),
            P(),
            P("ep", None),
            P("ep", None),
            P("ep", None, "tp"),
            P("ep", None, "tp"),
            P("ep", "tp", None),
        ),
        out_specs=(P("ep", "tp"), P(("ep", "tp"), None)),
        check_vma=False,
    )
```

```python
import functools
import math

import jax
import jax.numpy as jnp
import numpy as np
from jax import lax
from jax.experimental import pallas as pl
from jax.experimental.pallas import tpu as pltpu
from jax.sharding import PartitionSpec as P

EPS = 1e-06
THETA = 500000.0


def rms_norm(values, norm_gain):
    return values * lax.rsqrt(jnp.mean(values * values, axis=-1, keepdims=True) + EPS) * norm_gain


def rope_tables(positions, rope_dim):
    freqs = 1.0 / THETA ** (jnp.arange(0, rope_dim, 2, dtype=jnp.float32) / rope_dim)
    angles = positions.astype(jnp.float32)[:, None] * freqs[None, :]
    return (jnp.cos(angles), jnp.sin(angles))


def rotate(values, rot_cos, rot_sin):
    half_dim = values.shape[-1] // 2
    first_half = values[..., :half_dim]
    second_half = values[..., half_dim:]
    return jnp.concatenate(
        [
            first_half * rot_cos - second_half * rot_sin,
            second_half * rot_cos + first_half * rot_sin,
        ],
        axis=-1,
    )

MESH = pl.DeviceIdType.MESH
VMEM = pltpu.VMEM


def remote(src, dst, send, recv, device):
    return pltpu.make_async_remote_copy(
        src_ref=src, dst_ref=dst, send_sem=send, recv_sem=recv, device_id=device, device_id_type=MESH
    )


def greet(me, quarter, n_ep, highs):
    high, low = quarter // 2, quarter % 2
    barrier = pltpu.get_barrier_semaphore()

    def hello(device):
        pl.semaphore_signal(barrier, inc=1, device_id=device, device_id_type=MESH)

    def hello_ep(step, carry):
        hello((lax.rem(me + step, n_ep), quarter))
        return carry

    lax.fori_loop(1, n_ep, hello_ep, 0)
    hello((me, high * 2 + 1 - low))
    for step in range(1, highs):
        hello((me, lax.rem(high + step, highs) * 2 + low))
    pl.semaphore_wait(barrier, n_ep - 1 + 1 + highs - 1)


def spread_kernel(
    n_ep, highs, rows_ref, lat_ref, arrived, lat_all,
    own_sem, ep_send, ep_recv, high_send, high_recv, low_send, low_recv,
):
    me, quarter = lax.axis_index("ep"), lax.axis_index("tp")
    high, low = quarter // 2, quarter % 2
    partner = (me, high * 2 + 1 - low)
    greet(me, quarter, n_ep, highs)
    payloads = (
        (lambda j: rows_ref.at[j], arrived),
        (lambda j: lat_ref, lat_all),
    )
    own = [
        pltpu.make_async_copy(outgoing(me), into.at[low, high, me], own_sem.at[p])
        for p, (outgoing, into) in enumerate(payloads)
    ]
    for copy in own:
        copy.start()

    def ep_copy(p, step):
        outgoing, into = payloads[p]
        j = lax.rem(me + step, n_ep)
        return remote(
            outgoing(j), into.at[low, high, me], ep_send.at[p, step], ep_recv.at[p, step], (j, quarter)
        )

    def ep_arrival(p, step):
        outgoing, into = payloads[p]
        j = lax.rem(me + n_ep - step, n_ep)
        return remote(
            outgoing(me), into.at[low, high, j], ep_send.at[p, step], ep_recv.at[p, step], (j, quarter)
        )

    def high_copy(p, step, hop):
        into = payloads[p][1]
        j = lax.rem(me + n_ep - step, n_ep)
        block = into.at[low, high, j]
        return remote(
            block, block, high_send.at[p, hop, step], high_recv.at[p, hop, step],
            (me, lax.rem(high + hop, highs) * 2 + low),
        )

    def high_arrival(p, step, hop):
        into = payloads[p][1]
        j = lax.rem(me + n_ep - step, n_ep)
        block = into.at[low, lax.rem(high + highs - hop, highs), j]
        return remote(
            block, block, high_send.at[p, hop, step], high_recv.at[p, hop, step],
            (me, lax.rem(high + hop, highs) * 2 + low),
        )

    def low_copy(p, step, hop, side):
        into = payloads[p][1]
        j = lax.rem(me + n_ep - step, n_ep)
        block = into.at[side, lax.rem(high + highs - hop, highs), j]
        return remote(block, block, low_send.at[p, hop, step], low_recv.at[p, hop, step], partner)

    def start_ep(step, carry, p):
        ep_copy(p, step).start()
        return carry

    def forward(step, carry, p):
        ep_arrival(p, step).wait_recv()
        for hop in range(1, highs):
            high_copy(p, step, hop).start()
        low_copy(p, step, 0, low).start()
        return carry

    def forward_low(step, carry, p):
        for hop in range(1, highs):
            high_arrival(p, step, hop).wait_recv()
            low_copy(p, step, hop, low).start()
        return carry

    def finish(step, carry, p):
        for hop in range(highs):
            low_copy(p, step, hop, 1 - low).wait_recv()
            low_copy(p, step, hop, low).wait_send()
        for hop in range(1, highs):
            high_copy(p, step, hop).wait_send()
        return carry

    def finish_ep(step, carry, p):
        ep_copy(p, step).wait_send()
        return carry

    for p in range(2):
        lax.fori_loop(1, n_ep, functools.partial(start_ep, p=p), 0)
    for p in range(2):
        own[p].wait()
        for hop in range(1, highs):
            high_copy(p, 0, hop).start()
        low_copy(p, 0, 0, low).start()
        lax.fori_loop(1, n_ep, functools.partial(forward, p=p), 0)
    for p in range(2):
        lax.fori_loop(0, n_ep, functools.partial(forward_low, p=p), 0)
    for p in range(2):
        lax.fori_loop(0, n_ep, functools.partial(finish, p=p), 0)
        lax.fori_loop(1, n_ep, functools.partial(finish_ep, p=p), 0)


def spread(rows, lat, quarters):
    n_ep, cap, model_dim = rows.shape
    highs = quarters // 2
    dma = pltpu.SemaphoreType.DMA
    return pl.pallas_call(
        functools.partial(spread_kernel, n_ep, highs),
        out_shape=(
            jax.ShapeDtypeStruct((2, highs, n_ep, cap, model_dim), rows.dtype),
            jax.ShapeDtypeStruct((2, highs, n_ep) + lat.shape, lat.dtype),
        ),
        in_specs=[pl.BlockSpec(memory_space=VMEM)] * 2,
        out_specs=(pl.BlockSpec(memory_space=VMEM),) * 2,
        scratch_shapes=[
            dma((2,)),
            dma((2, n_ep)),
            dma((2, n_ep)),
            dma((2, highs, n_ep)),
            dma((2, highs, n_ep)),
            dma((2, highs, n_ep)),
            dma((2, highs, n_ep)),
        ],
        compiler_params=pltpu.CompilerParams(
            collective_id=0, has_side_effects=True, vmem_limit_bytes=60 << 20
        ),
        name="spread",
    )(rows, lat)


def collect_kernel(
    n_ep, highs, part_ref, ret, low_buf, high_buf, sum_buf, final_buf,
    low_send, low_recv, high_send, high_recv, ep_send, ep_recv,
):
    me, quarter = lax.axis_index("ep"), lax.axis_index("tp")
    high, low = quarter // 2, quarter % 2
    partner = (me, high * 2 + 1 - low)
    greet(me, quarter, n_ep, highs)

    def low_copy(step):
        j = lax.rem(me + step, n_ep)
        return remote(
            part_ref.at[1 - low, j], low_buf.at[j], low_send.at[step], low_recv.at[step], partner
        )

    def high_copy(step, hop):
        j = lax.rem(me + step, n_ep)
        other = lax.rem(high + hop, highs)
        return remote(
            sum_buf.at[j, other], high_buf.at[hop, j], high_send.at[hop, step],
            high_recv.at[hop, step], (me, other * 2 + low),
        )

    def ep_copy(step):
        j = lax.rem(me + step, n_ep)
        return remote(final_buf.at[j], ret.at[me], ep_send.at[step], ep_recv.at[step], (j, quarter))

    def ep_arrival(step):
        j = lax.rem(me + n_ep - step, n_ep)
        return remote(final_buf.at[j], ret.at[j], ep_send.at[step], ep_recv.at[step], (j, quarter))

    def start_low(step, carry):
        low_copy(step).start()
        return carry

    def add_low(step, carry):
        low_copy(step).wait_recv()
        j = lax.rem(me + step, n_ep)
        sum_buf[j] = (
            part_ref[low, j].astype(jnp.float32) + low_buf[j].astype(jnp.float32)
        ).astype(jnp.bfloat16)
        for hop in range(1, highs):
            high_copy(step, hop).start()
        return carry

    def total(step):
        j = lax.rem(me + step, n_ep)
        value = part_ref[low, j, high].astype(jnp.float32) + low_buf[j, high].astype(jnp.float32)
        for hop in range(1, highs):
            high_copy(step, hop).wait_recv()
            value = value + high_buf[hop, j].astype(jnp.float32)
        return value.astype(jnp.bfloat16)

    def add_high(step, carry):
        final_buf[lax.rem(me + step, n_ep)] = total(step)
        ep_copy(step).start()
        return carry

    def finish(step, carry):
        ep_arrival(step).wait_recv()
        ep_copy(step).wait_send()
        return carry

    def finish_tp(step, carry):
        low_copy(step).wait_send()
        for hop in range(1, highs):
            high_copy(step, hop).wait_send()
        return carry

    lax.fori_loop(1, n_ep, start_low, 0)
    low_copy(0).start()
    lax.fori_loop(1, n_ep, add_low, 0)
    add_low(0, 0)
    lax.fori_loop(1, n_ep, add_high, 0)
    ret[me] = total(0)
    lax.fori_loop(1, n_ep, finish, 0)
    lax.fori_loop(0, n_ep, finish_tp, 0)


def collect(partial):
    _, n_ep, highs, cap, model_dim = partial.shape
    dma = pltpu.SemaphoreType.DMA
    kind = partial.dtype
    return pl.pallas_call(
        functools.partial(collect_kernel, n_ep, highs),
        out_shape=jax.ShapeDtypeStruct((n_ep, cap, model_dim), kind),
        in_specs=[pl.BlockSpec(memory_space=VMEM)],
        out_specs=pl.BlockSpec(memory_space=VMEM),
        scratch_shapes=[
            VMEM((n_ep, highs, cap, model_dim), kind),
            VMEM((highs, n_ep, cap, model_dim), kind),
            VMEM((n_ep, highs, cap, model_dim), kind),
            VMEM((n_ep, cap, model_dim), kind),
            dma((n_ep,)),
            dma((n_ep,)),
            dma((highs, n_ep)),
            dma((highs, n_ep)),
            dma((n_ep,)),
            dma((n_ep,)),
        ],
        compiler_params=pltpu.CompilerParams(
            collective_id=1, has_side_effects=True, vmem_limit_bytes=62 << 20
        ),
        name="collect",
    )(partial)


def attend_kernel(
    heads, nope_dim, value_dim, latent_dim, scale,
    lat_ref, wk_ref, wv_ref, qn_ref, qr_ref, kg_ref, og_ref, out_ref, acc, den,
):
    block = pl.program_id(0)
    block_rows = lat_ref.shape[0]
    tok_rows = qn_ref.shape[1]
    offset = lax.axis_index("ep") * tok_rows
    first = block * block_rows

    @pl.when(block == 0)
    def _():
        acc[...] = jnp.zeros_like(acc)
        den[...] = jnp.zeros_like(den)

    @pl.when(first <= offset + tok_rows - 1)
    def _():
        latent = lat_ref[:, :latent_dim]
        rot_key = lat_ref[:, latent_dim:]
        keys = jnp.dot(latent, wk_ref[...], preferred_element_type=jnp.float32)
        values = jnp.dot(latent, wv_ref[...], preferred_element_type=jnp.float32).astype(jnp.bfloat16)
        shape = (tok_rows, block_rows)
        visible = offset + lax.broadcasted_iota(jnp.int32, shape, 0) >= first + lax.broadcasted_iota(
            jnp.int32, shape, 1
        )
        across = (((1,), (1,)), ((), ()))
        for head in range(heads):
            key = keys[:, head * nope_dim : (head + 1) * nope_dim]
            key = rms_norm(key, kg_ref[...]).astype(jnp.bfloat16)
            scores = lax.dot_general(qn_ref[head], key, across, preferred_element_type=jnp.float32)
            scores = scores + lax.dot_general(
                qr_ref[head], rot_key, across, preferred_element_type=jnp.float32
            )
            weights = jnp.where(visible, jnp.exp(scores * scale), 0.0)
            den[head] += jnp.sum(weights, axis=-1, keepdims=True)
            acc[head] += jnp.dot(
                weights.astype(jnp.bfloat16),
                values[:, head * value_dim : (head + 1) * value_dim],
                preferred_element_type=jnp.float32,
            )

    @pl.when(block == pl.num_programs(0) - 1)
    def _():
        for head in range(heads):
            mixed = rms_norm(acc[head] / den[head], og_ref[...])
            out_ref[:, head * value_dim : (head + 1) * value_dim] = mixed.astype(jnp.bfloat16)


def attend(lat_rows, w_key_up, w_value_up, query_nope, query_rope, key_gain, out_gain):
    heads, tok_rows, nope_dim = query_nope.shape
    rope_dim = query_rope.shape[2]
    value_dim = out_gain.shape[0]
    total, width = lat_rows.shape
    block_rows = math.gcd(total, 512)
    whole = pl.BlockSpec(memory_space=VMEM)
    return pl.pallas_call(
        functools.partial(
            attend_kernel, heads, nope_dim, value_dim, width - rope_dim, (nope_dim + rope_dim) ** (-0.5)
        ),
        grid=(total // block_rows,),
        out_shape=jax.ShapeDtypeStruct((tok_rows, heads * value_dim), jnp.bfloat16),
        in_specs=[pl.BlockSpec((block_rows, width), lambda b: (b, 0))] + [whole] * 6,
        out_specs=pl.BlockSpec((tok_rows, heads * value_dim), lambda b: (0, 0)),
        scratch_shapes=[
            VMEM((heads, tok_rows, value_dim), jnp.float32),
            VMEM((heads, tok_rows, 1), jnp.float32),
        ],
        name="attend",
    )(
        lat_rows, w_key_up, w_value_up, query_nope, query_rope,
        key_gain.reshape(1, -1), out_gain.reshape(1, -1),
    )


LANES = 128
TILE = 256


def layer_kernel(
    n_ep, heads, nope_dim, rope_dim, value_dim,
    tok_hbm, mg_hbm, routes_hbm, rw_hbm, kv_hbm, rk_hbm, freq_hbm, lg_hbm, rg_hbm, q_hbm, qg_hbm,
    wk_hbm, wv_hbm, kg_hbm, og_hbm, wg_hbm, wu_hbm, wd_hbm,
    att_ref, moe_ref,
    tok_ref, mg_ref, routes_ref, rw_ref, kv_ref, rk_ref, freq_ref, lg_ref, rg_ref, q_ref, qg_ref,
    wk_ref, wv_ref, kg_ref, og_ref,
    wgu, wd, normed, rows_out, arrived, hid, part, low_buf, sum_buf, high_buf, final_buf, ret, hits,
    lat_all, cos_ref, sin_ref, qn, qr, acc, den,
    in_sem, w_sem, ep_send, ep_recv, high_send, high_recv, low_send, low_recv,
    rlow_send, rlow_recv, rhigh_send, rhigh_recv, rep_send, rep_recv,
    lz_send, lz_recv, ly_send, ly_recv, ll_send, ll_recv,
):
    me, quarter = lax.axis_index("ep"), lax.axis_index("tp")
    n_z = n_ep // 2
    z, y = me // 2, lax.rem(me, 2)
    high, low = quarter // 2, lax.rem(quarter, 2)
    partner = (me, high * 2 + 1 - low)
    across = (me, (1 - high) * 2 + low)
    bf16, f32 = jnp.bfloat16, jnp.float32
    cap = rows_out.shape[1]
    model_dim = rows_out.shape[2]
    tok_rows = tok_ref.shape[0]
    part_rows = tok_rows // 4
    ff = wd.shape[0]
    half = tok_rows // 2
    barrier = pltpu.get_barrier_semaphore()

    def hello(device):
        pl.semaphore_signal(barrier, inc=1, device_id=device, device_id_type=MESH)

    def hello_ep(step, carry):
        hello((lax.rem(me + step, n_ep), quarter))
        return carry

    lax.fori_loop(1, n_ep, hello_ep, 0)
    hello(partner)
    hello(across)

    def weight_copies():
        out = []
        for i in range(ff // LANES):
            out.append((wg_hbm.at[0, :, pl.ds(LANES * i, LANES)], wgu.at[:, pl.ds(TILE * i, LANES)]))
            out.append((wu_hbm.at[0, :, pl.ds(LANES * i, LANES)], wgu.at[:, pl.ds(TILE * i + LANES, LANES)]))
        out.append((wd_hbm.at[0], wd))
        return [pltpu.make_async_copy(a, b, w_sem.at[i]) for i, (a, b) in enumerate(out)]

    sources = (
        tok_hbm, mg_hbm, routes_hbm, rw_hbm, kv_hbm, rk_hbm, freq_hbm, lg_hbm, rg_hbm, q_hbm, qg_hbm,
        wk_hbm, wv_hbm, kg_hbm, og_hbm,
    )
    loaded = (
        tok_ref, mg_ref, routes_ref, rw_ref, kv_ref, rk_ref, freq_ref, lg_ref, rg_ref, q_ref, qg_ref,
        wk_ref, wv_ref, kg_ref, og_ref,
    )
    loads = [
        pltpu.make_async_copy(source, into, in_sem.at[i])
        for i, (source, into) in enumerate(zip(sources, loaded))
    ]
    for copy in loads:
        copy.start()
    def ep_to(s, t):
        return lax.rem(z + s, n_z) * 2 + lax.rem(y + t, 2)

    def ep_from(s, t):
        return lax.rem(z + n_z - s, n_z) * 2 + lax.rem(y + t, 2)


    tokens = (1, tok_rows)
    token = lax.broadcasted_iota(jnp.int32, tokens, 1)

    def quarter_of(index):
        return sum((index >= q * part_rows).astype(jnp.int32) for q in range(1, 4))

    def hit_matrix(count, places):
        slot = lax.broadcasted_iota(jnp.int32, (count, places[0].shape[1]), 0).astype(f32)
        return sum((slot == place).astype(f32) for place in places)

    def gather_rows(select, into):
        select = select.astype(bf16)
        wide = 512
        for n in range(model_dim // wide):
            cols = slice(n * wide, (n + 1) * wide)
            rows = jnp.dot(select, normed[:, cols], preferred_element_type=f32).astype(bf16)
            into(cols, rows, wide)

    def own_part(row):
        return sum(
            jnp.where(quarter == q, row[:, q * part_rows : (q + 1) * part_rows], 0.0) for q in range(4)
        )

    def ranks():
        shape = (tok_rows, tok_rows)
        before, after = lax.broadcasted_iota(jnp.int32, shape, 0), lax.broadcasted_iota(jnp.int32, shape, 1)
        earlier = ((before < after) & (quarter_of(before) == quarter_of(after))).astype(bf16)
        experts = lax.broadcasted_iota(jnp.int32, (n_ep, tok_rows), 0)
        ones = [(routes_ref[k : k + 1, :] == experts).astype(f32) for k in range(2)]
        rank = jnp.dot((ones[0] + ones[1]).astype(bf16), earlier, preferred_element_type=f32)
        return [jnp.sum(rank * one, axis=0, keepdims=True) for one in ones]

    def norm_tokens():
        step = 64
        for i in range(tok_rows // step):
            rows = tok_ref[i * step : (i + 1) * step, :].astype(f32)
            normed[i * step : (i + 1) * step, :] = rms_norm(rows, mg_ref[...]).astype(bf16)

    def dispatch(rank):
        mine = quarter_of(token) == quarter
        places = [
            jnp.where(mine, routes_ref[k : k + 1, :].astype(f32) * cap + rank[k], -1.0) for k in range(2)
        ]

        def into(cols, rows, wide):
            rows_out[:, :, cols] = rows.reshape(n_ep, cap, wide)

        gather_rows(hit_matrix(n_ep * cap, places), into)

    def own_dispatch(rank):
        number = quarter_of(token)
        position = lax.rem(number, 2) * 2 + number // 2
        places = [
            jnp.where(routes_ref[k : k + 1, :] == me, position.astype(f32) * cap + rank[k], -1.0)
            for k in range(2)
        ]

        def into(cols, rows, wide):
            arrived[me, :, :, :, cols] = rows.reshape(2, 2, cap, wide)

        gather_rows(hit_matrix(4 * cap, places), into)

    def combine_matrices(rank):
        slot = lax.broadcasted_iota(jnp.int32, (n_ep * cap, part_rows), 0).astype(f32)
        weighted = jnp.zeros((n_ep * cap, part_rows), f32)
        for k in range(2):
            place = own_part(routes_ref[k : k + 1, :].astype(f32) * cap + rank[k])
            weighted += jnp.where(slot == place, own_part(rw_ref[k : k + 1, :]), 0.0)
        upper = weighted.astype(bf16)
        hits[0] = upper
        hits[1] = (weighted - upper.astype(f32)).astype(bf16)

    for copy in loads[:4]:
        copy.wait()
    for copy in weight_copies():
        copy.start()
    rank = ranks()
    norm_tokens()
    dispatch(rank)
    pl.semaphore_wait(barrier, n_ep + 1)

    def ep_copy(s, t):
        return remote(
            rows_out.at[ep_to(s, t)], arrived.at[me, low, high], ep_send.at[s, t], ep_recv.at[s, t],
            (ep_to(s, t), quarter),
        )

    def ep_arrival(s, t):
        j = ep_from(s, t)
        return remote(
            rows_out.at[j], arrived.at[j, low, high], ep_send.at[s, t], ep_recv.at[s, t], (j, quarter)
        )

    def high_copy(s, t, side):
        block = arrived.at[ep_from(s, t), low, side]
        return remote(block, block, high_send.at[s, t], high_recv.at[s, t], across)

    def low_copy(s, t, hop, side, core):
        block = arrived.at[ep_from(s, t), core, side]
        return remote(block, block, low_send.at[hop, s, t], low_recv.at[hop, s, t], partner)

    def each(s, body):
        for t in range(2):
            if t == 0:
                pl.when(s > 0)(functools.partial(body, s, 0))
            else:
                body(s, 1)

    def start_ep(s, carry):
        each(s, lambda s, t: ep_copy(s, t).start())
        return carry

    def order(i):
        if n_z % 2:
            return i
        return jnp.where(i < n_z - 1, lax.rem(2 * i, n_z - 1), n_z - 1)

    def send_rows(i):
        if i < n_z:
            start_ep(order(i), 0)

    start_ep(0, 0)
    send_rows(1)


    def lat_copy_z(k):
        block = lat_all.at[k, y, low]
        return remote(
            block, block, lz_send.at[k], lz_recv.at[k], (lax.rem(z + 1, n_z) * 2 + y, quarter)
        )

    def lat_copy_y(k, side):
        block = lat_all.at[k, side, low]
        return remote(block, block, ly_send.at[k], ly_recv.at[k], (z * 2 + 1 - y, quarter))

    def lat_copy_low(k, hop, core):
        block = lat_all.at[k, y if hop == 0 else 1 - y, core]
        return remote(block, block, ll_send.at[hop, k], ll_recv.at[hop, k], partner)

    def tables():
        half_dim = rope_dim // 2
        places = lax.broadcasted_iota(jnp.int32, (tok_rows, half_dim), 0) + me * tok_rows
        angles = places.astype(f32) * freq_ref[...]
        cos_ref[...] = jnp.cos(angles)
        sin_ref[...] = jnp.sin(angles)

    def lat_own():
        latent = rms_norm(kv_ref[...].astype(f32), lg_ref[...]).astype(bf16)
        raw = jnp.transpose(rk_ref[...].astype(f32))
        rot = rotate(rms_norm(raw, rg_ref[...]), cos_ref[...], sin_ref[...]).astype(bf16)
        step = lat_all.shape[3] - half
        for core in range(2):
            lat_all[z, y, core, :half] = latent[core * half : (core + 1) * half]
            first = core * half
            lat_all[z, y, core, half:] = jnp.concatenate(
                [rot[first + i : first + i + step] for i in range(0, half, step)], axis=1
            )

    def lat_send():
        pl.when(z < n_z - 1)(lambda: lat_copy_z(z).start())
        pl.when(y == 0)(lambda: lat_copy_y(z, y).start())

    def lat_step(k, carry):
        origin = z - k

        @pl.when(origin >= 0)
        def _():
            lat_copy_z(origin).wait_recv()
            pl.when(z < n_z - 1)(lambda: lat_copy_z(origin).start())
            lat_copy_y(origin, y).start()
            lat_copy_low(origin, 0, low).start()

        return carry

    def lat_side(k, carry):
        origin = z - k

        @pl.when((origin >= 0) & (k + y > 0))
        def _():
            lat_copy_y(origin, 1 - y).wait_recv()
            lat_copy_low(origin, 1, low).start()

        return carry


    def queries():
        raw = q_ref[...].astype(f32)
        width = nope_dim + rope_dim
        for head in range(heads):
            query = rms_norm(raw[:, head * width : (head + 1) * width], qg_ref[...])
            qn[head] = query[:, :nope_dim].astype(bf16)
            qr[head] = rotate(query[:, nope_dim:], cos_ref[...], sin_ref[...]).astype(bf16)

    scale = (nope_dim + rope_dim) ** (-0.5)

    def attend_block(zj, yj, own):
        latent = lat_all[zj, yj, :, :half].reshape(tok_rows, lat_all.shape[-1])
        rot_key = jnp.concatenate(
            [
                lat_all[zj, yj, core, half:, i : i + rope_dim]
                for core in range(2)
                for i in range(0, lat_all.shape[-1], rope_dim)
            ],
            axis=0,
        )
        keys = jnp.dot(latent, wk_ref[...], preferred_element_type=f32)
        values = jnp.dot(latent, wv_ref[...], preferred_element_type=f32).astype(bf16)
        lined = (((1,), (1,)), ((), ()))
        for head in range(heads):
            key = rms_norm(keys[:, head * nope_dim : (head + 1) * nope_dim], kg_ref[...]).astype(bf16)
            scores = lax.dot_general(qn[head], key, lined, preferred_element_type=f32)
            scores = scores + lax.dot_general(qr[head], rot_key, lined, preferred_element_type=f32)
            weights = jnp.exp(scores * scale)
            if own:
                shape = (tok_rows, tok_rows)
                visible = lax.broadcasted_iota(jnp.int32, shape, 0) >= lax.broadcasted_iota(jnp.int32, shape, 1)
                weights = jnp.where(visible, weights, 0.0)
            total = jnp.sum(weights, axis=-1, keepdims=True)
            mixed = jnp.dot(
                weights.astype(bf16), values[:, head * value_dim : (head + 1) * value_dim],
                preferred_element_type=f32,
            )
            if own:
                den[head] = total
                acc[head] = mixed
            else:
                den[head] += total
                acc[head] += mixed

    def attend_side(k):
        @pl.when((z >= k) & (k + y > 0))
        def _():
            lat_copy_low(z - k, 1, 1 - low).wait_recv()
            attend_block(z - k, 1 - y, False)

    def attend_line(k):
        @pl.when(z >= k)
        def _():
            lat_copy_low(z - k, 0, 1 - low).wait_recv()
            attend_block(z - k, y, False)


    def forward(s, t):
        ep_arrival(s, t).wait_recv()
        high_copy(s, t, high).start()
        low_copy(s, t, 0, high, low).start()

    def forward_low(s, t):
        high_copy(s, t, 1 - high).wait_recv()
        low_copy(s, t, 1, 1 - high, low).start()

    def arrive(s, t):
        low_copy(s, t, 0, high, 1 - low).wait_recv()
        low_copy(s, t, 1, 1 - high, 1 - low).wait_recv()

    def expert_up(s):
        first = lax.rem(z + n_z - s, n_z) * 2
        rows = arrived[pl.ds(first, 2)].reshape(8 * cap, model_dim)
        for i in range(ff // LANES):
            both = jnp.dot(rows, wgu[:, TILE * i : TILE * (i + 1)], preferred_element_type=f32)
            gate, upward = both[:, :LANES], both[:, LANES:]
            hid[:, LANES * i : LANES * (i + 1)] = (jax.nn.silu(gate) * upward).astype(bf16)

    def expert_down(s):
        first = lax.rem(z + n_z - s, n_z) * 2
        for n in range(model_dim // TILE):
            down = jnp.dot(hid[...], wd[:, TILE * n : TILE * (n + 1)], preferred_element_type=f32)
            part[pl.ds(first, 2), :, :, :, TILE * n : TILE * (n + 1)] = down.astype(bf16).reshape(
                2, 2, 2, cap, TILE
            )

    def rlow_copy(s, t):
        j = ep_from(s, t)
        return remote(part.at[j, 1 - low], low_buf.at[j], rlow_send.at[s, t], rlow_recv.at[s, t], partner)

    def rhigh_copy(s, t):
        j = ep_from(s, t)
        return remote(sum_buf.at[j], high_buf.at[j], rhigh_send.at[s, t], rhigh_recv.at[s, t], across)

    def rep_copy(s, t):
        j = ep_from(s, t)
        return remote(final_buf.at[j], ret.at[me], rep_send.at[s, t], rep_recv.at[s, t], (j, quarter))

    def rep_arrival(s, t):
        j = ep_to(s, t)
        return remote(final_buf.at[j], ret.at[j], rep_send.at[s, t], rep_recv.at[s, t], (j, quarter))

    def reduce_low(s, t):
        j = ep_from(s, t)
        rlow_copy(s, t).wait_recv()
        sum_buf[j] = (part[j, low, 1 - high].astype(f32) + low_buf[j, 1 - high].astype(f32)).astype(bf16)
        rhigh_copy(s, t).start()

    def reduce_high(s, t):
        j = ep_from(s, t)
        rhigh_copy(s, t).wait_recv()
        value = part[j, low, high].astype(f32) + low_buf[j, high].astype(f32) + high_buf[j].astype(f32)
        if isinstance(s, int) and s + t == 0:
            ret[me] = value.astype(bf16)
        else:
            final_buf[j] = value.astype(bf16)
            rep_copy(s, t).start()

    def both(body, s):
        body(s, 0)
        body(s, 1)

    def lat_hop(k):
        if k < n_z:
            lat_step(k, 0)

    def attend_step(k):
        if k < n_z:
            if k > 0:
                attend_line(k)
            attend_side(k)

    own_dispatch(rank)
    combine_matrices(rank)
    for copy in loads[4:]:
        copy.wait()
    tables()
    forward(0, 1)
    lat_own()
    queries()
    attend_block(z, y, True)

    first, before, between, after = {}, {}, {}, {}

    def at(table, i, body, *args):
        table.setdefault(i, []).append(functools.partial(body, *args))

    def weights_here():
        for copy in weight_copies():
            copy.wait()

    last = n_z - 1
    at(before, 0, weights_here)
    at(before, 0, send_rows, 2)
    at(between, 0, lambda: both(forward, order(1)))
    for i in range(3, n_z):
        at(after, 0, send_rows, i)
    at(first, 1, lambda: both(forward, order(2)))
    at(after, 0, lat_send)
    for i in range(1, last):
        if i + 2 <= last:
            at(between, i, lambda i=i: forward(order(i + 2), 0))
            at(between, i + 1, lambda i=i: forward(order(i + 2), 1))
        at(after, i, lambda i=i: both(reduce_low, order(i)))
        if i > 1:
            at(after, i, lambda i=i: both(reduce_high, order(i - 1)))
    at(after, 1, lat_hop, 1)
    at(after, 2, lat_hop, 2)
    at(between, last, reduce_low, 0, 1)
    at(between, last, lat_side, 0, 0)
    at(between, last, lat_side, 1, 0)

    def run(table, i):
        for place, bodies in table.items():

            @pl.when(i == place)
            def _():
                for body in bodies:
                    body()

    def stage(i, carry):
        s = order(i)
        each(s, forward_low)
        run(first, i)
        each(s, arrive)
        run(before, i)
        expert_up(s)
        run(between, i)
        expert_down(s)
        for t in range(2):
            rlow_copy(s, t).start()
        run(after, i)
        return carry

    lax.fori_loop(0, n_z, stage, 0)
    both(reduce_low, order(last))
    reduce_low(0, 0)
    both(reduce_high, order(last - 1))
    attend_step(0)
    attend_step(1)
    lat_side(2, 0)
    for far in range(3, n_z):
        lat_hop(far)
    both(reduce_high, order(last))
    reduce_high(0, 1)
    reduce_high(0, 0)
    for far in range(3, n_z):
        lat_side(far, 0)
    for far in range(2, n_z):
        attend_step(far)
    for head in range(heads):
        mixed = rms_norm(acc[head] / den[head], og_ref[...])
        att_ref[:, head * value_dim : (head + 1) * value_dim] = mixed.astype(bf16)

    def returned(s, carry):
        each(s, lambda s, t: rep_arrival(s, t).wait_recv())
        return carry

    lax.fori_loop(0, n_z, returned, 0)
    wide = 512
    lined = (((0,), (0,)), ((), ()))
    for n in range(model_dim // wide):
        values = ret[:, :, n * wide : (n + 1) * wide].reshape(n_ep * cap, wide)
        mixed = lax.dot_general(hits[0], values, lined, preferred_element_type=f32)
        mixed += lax.dot_general(hits[1], values, lined, preferred_element_type=f32)
        moe_ref[:, n * wide : (n + 1) * wide] = mixed.astype(bf16)

    def sent(s, carry):
        def rows_sent(s, t):
            ep_copy(s, t).wait_send()
            high_copy(s, t, high).wait_send()
            low_copy(s, t, 0, high, low).wait_send()
            low_copy(s, t, 1, 1 - high, low).wait_send()
            rep_copy(s, t).wait_send()

        each(s, rows_sent)
        for t in range(2):
            rlow_copy(s, t).wait_send()
            rhigh_copy(s, t).wait_send()

        origin = z - s

        @pl.when(origin >= 0)
        def _():
            pl.when(z < n_z - 1)(lambda: lat_copy_z(origin).wait_send())
            pl.when((s > 0) | (y == 0))(lambda: lat_copy_y(origin, y).wait_send())
            pl.when(s > 0)(lambda: lat_copy_low(origin, 0, low).wait_send())
            pl.when(s + y > 0)(lambda: lat_copy_low(origin, 1, low).wait_send())

        return carry

    lax.fori_loop(0, n_z, sent, 0)


def layer(
    queries, kv_latent, rope_key, latent_gain, w_key_up, w_value_up, query_gain, key_gain,
    rope_gain, out_gain, moe_tokens, moe_gain, routes, route_weights, w_gate, w_up, w_down, n_ep, cap,
):
    tok_rows = queries.shape[0]
    nope_dim, rope_dim, value_dim = key_gain.shape[0], rope_key.shape[1], out_gain.shape[0]
    heads = w_key_up.shape[1] // nope_dim
    model_dim = moe_tokens.shape[1]
    part_rows = tok_rows // 4
    ff = w_down.shape[1]
    n_z = n_ep // 2
    packed = tok_rows // 2 * rope_dim // kv_latent.shape[1]
    dma = pltpu.SemaphoreType.DMA
    kind, f32 = jnp.bfloat16, jnp.float32
    pairs = (n_z, 2)
    block = (cap, model_dim)
    freqs = (1.0 / THETA ** (np.arange(0, rope_dim, 2) / rope_dim)).astype(np.float32)
    small = (
        moe_tokens, moe_gain.reshape(1, -1), routes.T, route_weights.T, kv_latent, rope_key.T,
        freqs.reshape(1, -1), latent_gain.reshape(1, -1), rope_gain.reshape(1, -1), queries,
        query_gain.reshape(1, -1), w_key_up, w_value_up, key_gain.reshape(1, -1), out_gain.reshape(1, -1),
    )
    return pl.pallas_call(
        functools.partial(layer_kernel, n_ep, heads, nope_dim, rope_dim, value_dim),
        out_shape=(
            VMEM((tok_rows, heads * value_dim), kind),
            VMEM((part_rows, model_dim), kind),
        ),
        in_specs=[pl.BlockSpec(memory_space=pltpu.HBM)] * (len(small) + 3),
        out_specs=(pl.BlockSpec(memory_space=VMEM),) * 2,
        scratch_shapes=[VMEM(array.shape, array.dtype) for array in small] + [
            VMEM((model_dim, 2 * ff), kind),
            VMEM((ff, model_dim), kind),
            VMEM((tok_rows, model_dim), kind),
            VMEM((n_ep,) + block, kind),
            VMEM((n_ep, 2, 2) + block, kind),
            VMEM((8 * cap, ff), kind),
            VMEM((n_ep, 2, 2) + block, kind),
            VMEM((n_ep, 2) + block, kind),
            VMEM((n_ep,) + block, kind),
            VMEM((n_ep,) + block, kind),
            VMEM((n_ep,) + block, kind),
            VMEM((n_ep,) + block, kind),
            VMEM((2, n_ep * cap, part_rows), kind),
            VMEM((n_z, 2, 2, tok_rows // 2 + packed, kv_latent.shape[1]), kind),
            VMEM((tok_rows, rope_dim // 2), f32),
            VMEM((tok_rows, rope_dim // 2), f32),
            VMEM((heads, tok_rows, nope_dim), kind),
            VMEM((heads, tok_rows, rope_dim), kind),
            VMEM((heads, tok_rows, value_dim), f32),
            VMEM((heads, tok_rows, 1), f32),
            dma((len(small),)),
            dma((2 * (ff // LANES) + 1,)),
            dma(pairs), dma(pairs), dma(pairs), dma(pairs), dma((2,) + pairs), dma((2,) + pairs),
            dma(pairs), dma(pairs), dma(pairs), dma(pairs), dma(pairs), dma(pairs),
            dma((n_z,)), dma((n_z,)), dma((n_z,)), dma((n_z,)), dma((2, n_z)), dma((2, n_z)),
        ],
        compiler_params=pltpu.CompilerParams(
            collective_id=2, has_side_effects=True, vmem_limit_bytes=62 << 20
        ),
        name="layer",
    )(*small, w_gate, w_up, w_down)


def on_device(
    queries,
    kv_latent,
    rope_key,
    latent_gain,
    w_key_up,
    w_value_up,
    query_gain,
    key_gain,
    rope_gain,
    out_gain,
    moe_tokens,
    moe_gain,
    routes,
    route_weights,
    w_gate,
    w_up,
    w_down,
):
    quarters = lax.axis_size("tp")
    n_ep = lax.axis_size("ep")
    my_part = lax.axis_index("tp")
    tok_rows = queries.shape[0]
    nope_dim = key_gain.shape[0]
    value_dim = out_gain.shape[0]
    rope_dim = rope_key.shape[1]
    head_count = w_key_up.shape[1] // nope_dim
    positions = lax.axis_index("ep") * tok_rows + jnp.arange(tok_rows, dtype=jnp.int32)
    rot_cos, rot_sin = rope_tables(positions, rope_dim)
    n_rows, model_dim = moe_tokens.shape
    top_count = routes.shape[1]
    part_rows = n_rows // quarters
    experts = n_ep * w_gate.shape[0]
    capacity = (3 * top_count * part_rows + 2 * experts - 1) // (2 * experts)
    one_kernel = quarters == 4 and n_ep % 2 == 0 and w_gate.shape[0] == 1 and top_count == 2
    lat_parts = kv_latent.shape[1] // rope_dim
    one_kernel = one_kernel and n_ep >= 8 and kv_latent.shape[1] % LANES == 0
    one_kernel = one_kernel and kv_latent.shape[1] % rope_dim == 0 and n_rows % (32 * lat_parts) == 0
    if one_kernel and capacity % 8 == 0 and w_down.shape[1] % LANES == 0 and model_dim % 512 == 0:
        return layer(
            queries, kv_latent, rope_key, latent_gain, w_key_up, w_value_up, query_gain, key_gain, rope_gain,
            out_gain, moe_tokens, moe_gain, routes, route_weights, w_gate, w_up, w_down, n_ep, capacity,
        )
    lat_part = tok_rows // quarters

    def mine(values, rows):
        return lax.dynamic_slice_in_dim(values, my_part * rows, rows, 0)

    latent = rms_norm(mine(kv_latent, lat_part).astype(jnp.float32), latent_gain)
    rot_key = rotate(
        rms_norm(mine(rope_key, lat_part).astype(jnp.float32), rope_gain),
        mine(rot_cos, lat_part),
        mine(rot_sin, lat_part),
    )
    lat_own = jnp.concatenate([latent.astype(jnp.bfloat16), rot_key.astype(jnp.bfloat16)], axis=1)

    slot_count = experts * capacity
    own_rows = rms_norm(mine(moe_tokens, part_rows).astype(jnp.float32), moe_gain).astype(jnp.bfloat16)
    chosen = mine(routes, part_rows).reshape(part_rows * top_count)
    onehot = (chosen[:, None] == jnp.arange(experts, dtype=jnp.int32)).astype(jnp.float32)
    count = part_rows * top_count
    earlier = (jnp.arange(count)[:, None] > jnp.arange(count)[None, :]).astype(jnp.float32)
    rank = jnp.sum(jnp.dot(earlier, onehot) * onehot, axis=-1).astype(jnp.int32)
    slots = chosen * capacity + rank
    mine_hit = (slots[:, None] == jnp.arange(slot_count, dtype=jnp.int32)).astype(jnp.bfloat16)
    mine_hit = mine_hit.reshape(part_rows, top_count, slot_count)
    outgoing = jnp.einsum(
        "rs,rd->sd", jnp.sum(mine_hit, axis=1), own_rows, preferred_element_type=jnp.float32
    )
    outgoing = outgoing.astype(jnp.bfloat16).reshape(experts, capacity, model_dim)

    arrived, lat_all = spread(outgoing, lat_own, quarters)
    lat_rows = jnp.transpose(lat_all, (2, 1, 0, 3, 4)).reshape(n_ep * tok_rows, lat_own.shape[1])

    shape = arrived.shape
    gate = jnp.einsum("abecd,df->abecf", arrived, w_gate[0], preferred_element_type=jnp.float32)
    upward = jnp.einsum("abecd,df->abecf", arrived, w_up[0], preferred_element_type=jnp.float32)
    hidden = (jax.nn.silu(gate) * upward).astype(jnp.bfloat16)
    partial = jnp.einsum("abecf,fd->aebcd", hidden, w_down[0], preferred_element_type=jnp.float32)
    returned = collect(partial.astype(jnp.bfloat16))

    query = rms_norm(
        queries.astype(jnp.float32).reshape(tok_rows, head_count, nope_dim + rope_dim), query_gain
    )
    query_nope = query[..., :nope_dim].astype(jnp.bfloat16)
    query_rope = rotate(query[..., nope_dim:], rot_cos[:, None, :], rot_sin[:, None, :]).astype(
        jnp.bfloat16
    )
    attended = attend(
        lat_rows,
        w_key_up,
        w_value_up,
        jnp.transpose(query_nope, (1, 0, 2)),
        jnp.transpose(query_rope, (1, 0, 2)),
        key_gain,
        out_gain,
    )

    picked = jnp.einsum(
        "rks,sd->rkd",
        mine_hit,
        returned.reshape(slot_count, model_dim),
        preferred_element_type=jnp.float32,
    )
    own_weights = mine(route_weights, part_rows)
    moe_out = jnp.sum(picked * own_weights[:, :, None], axis=1).astype(jnp.bfloat16)
    return (attended, moe_out)


def solution(mesh):
    return jax.shard_map(
        on_device,
        mesh=mesh,
        in_specs=(
            P("ep", "tp"),
            P("ep", None),
            P("ep", None),
            P(),
            P(None, "tp"),
            P(None, "tp"),
            P(),
            P(),
            P(),
            P(),
            P("ep", None),
            P(),
            P("ep", None),
            P("ep", None),
            P("ep", None, "tp"),
            P("ep", None, "tp"),
            P("ep", "tp", None),
        ),
        out_specs=(P("ep", "tp"), P(("ep", "tp"), None)),
        check_vma=False,
    )
```
